512 devices in a mesh: ep: 32 (over z, x), tp: 16 (over y, core).
Axes of the slice: x: 4, y: 8, z: 8, core: 2. Of those that a mesh axis runs over, the one named last changes fastest.
Arguments:
- queries: bfloat16 [12288, 2048], P('ep', 'tp'), may hold values from -8 to 8
- keys: bfloat16 [12288, 2048], P('ep', 'tp'), may hold values from -8 to 8
- values: bfloat16 [12288, 2048], P('ep', 'tp'), may hold values from -6 to 6
- key_offset: bfloat16 [12288, 16], P('ep', 'tp'), may hold values from -15.25 to -0.4
- rows: bfloat16 [4096, 2048], P('ep'), may hold values from -6 to 6
- gain: float32 [2048], replicated, may hold values from 0.1 to 1.9
- gate_w: bfloat16 [32, 2048, 3584], P('ep', None, 'tp'), may hold values from -0.125 to 0.125
- up_w: bfloat16 [32, 2048, 3584], P('ep', None, 'tp'), may hold values from -0.125 to 0.125
- down_w: bfloat16 [32, 3584, 2048], P('ep', 'tp'), may hold values from -0.09375 to 0.09375
- expert_ids: int32 [4096, 2], P('ep'), may hold values from 0 to 31, all different within a row; in each aligned block of 128 rows (0 to 127, 128 to 255, ...) at most 16 rows name the same one
- route_weights: float32 [4096, 2], P('ep'), may hold values from 0.2 to 1
Outputs:
- attended: bfloat16 [12288, 2048], P('ep', 'tp')
- mixed: bfloat16 [4096, 2048], P('ep')
The draws below stay inside these ranges and needn't reach their ends.
Inputs may be any that keep to these rules, and one draw needn't show every extreme that they name: `expert_ids`: each token names 2 different experts; among the 128 tokens of one ep index no expert is chosen more than 16 times, and in some such block an expert is chosen exactly 16 times.
All inputs are finite; a program needn't handle non-finite values.
Results may differ from the reference program's by a relative error of at most 0.019.
Values may be sent and summed in bfloat16 or wider, within the bound.
No kernel may reach another device: no remote copies, remote signals or barrier semaphores. Data moves between devices by JAX's collectives and lax.ppermute only.
A program may use at most 128 MiB of HBM per device.

```python
import math
import jax
import jax.numpy as jnp
import numpy as np
from jax import lax

D = 2048
ATTENTION_HEADS = 16
HD = 128
FF = 3584
TOP = 2
TOK_A_DEV = 384
TOK_B_DEV = 128
EXPERTS = 32
SEQUENCE_TOKENS = 12288
TOKENS_B = 4096
CAP = 16
N_TP = 16


def unit_noise(noise_key, shape):
    return jax.random.normal(noise_key, shape, jnp.float32)


def stick_fields(key):
    groups = 16
    center_key, value_key, query_id_key, key_id_key, query_amp_key, key_amp_key, query_noise_key, key_noise_key, value_noise_key = jax.random.split(jax.random.fold_in(key, 23), 9)
    centers = jax.random.normal(center_key, (ATTENTION_HEADS, groups, HD), jnp.float32)
    centers = centers / jnp.sqrt(jnp.sum(centers * centers, axis=2, keepdims=True))
    value_centers = jax.random.normal(value_key, (ATTENTION_HEADS, groups, HD), jnp.float32)
    strength = (5.0 * HD ** 0.5) ** 0.5
    head_index = jnp.arange(ATTENTION_HEADS, dtype=jnp.int32)[None, :]
    query_group = jax.random.randint(query_id_key, (SEQUENCE_TOKENS, ATTENTION_HEADS), 0, groups)
    key_group = jax.random.randint(key_id_key, (SEQUENCE_TOKENS, ATTENTION_HEADS), 0, groups)
    query_amplitude = jax.random.uniform(query_amp_key, (SEQUENCE_TOKENS, ATTENTION_HEADS, 1), jnp.float32, 0.8, 1.2)
    key_amplitude = jax.random.uniform(key_amp_key, (SEQUENCE_TOKENS, ATTENTION_HEADS, 1), jnp.float32, 0.8, 1.2)
    shape = (SEQUENCE_TOKENS, ATTENTION_HEADS, HD)
    query_field = 1.2 * unit_noise(query_noise_key, shape) + strength * query_amplitude * centers[head_index, query_group]
    key_field = 1.2 * unit_noise(key_noise_key, shape) + strength * key_amplitude * centers[head_index, key_group]
    value_field = 0.6 * unit_noise(value_noise_key, shape) + 0.8 * value_centers[head_index, key_group]
    query_field = jnp.clip(query_field.reshape(SEQUENCE_TOKENS, ATTENTION_HEADS * HD), -8.0, 8.0)
    key_field = jnp.clip(key_field.reshape(SEQUENCE_TOKENS, ATTENTION_HEADS * HD), -8.0, 8.0)
    value_field = jnp.clip(value_field.reshape(SEQUENCE_TOKENS, ATTENTION_HEADS * HD), -6.0, 6.0)
    return (query_field, key_field, value_field)


def draw_queries(key, part):
    return stick_fields(key)[0].astype(jnp.bfloat16)


def draw_keys(key, part):
    return stick_fields(key)[1].astype(jnp.bfloat16)


def draw_values(key, part):
    return stick_fields(key)[2].astype(jnp.bfloat16)


def draw_key_offset(key, part):
    select_random_key, quick_random_key, gradual_random_key, offset_random_key, noise_random_key, spike_random_key, height_random_key = jax.random.split(jax.random.fold_in(key, 11), 7)
    slow_base = jax.random.uniform(gradual_random_key, (ATTENTION_HEADS,), jnp.float32, -14.0, -12.5)
    fast_base = jax.random.uniform(quick_random_key, (ATTENTION_HEADS,), jnp.float32, -8.0, -7.0)
    chosen = jax.random.uniform(select_random_key, (ATTENTION_HEADS,), jnp.float32) < 0.5
    base = jnp.where(chosen, fast_base, slow_base)
    blocks = SEQUENCE_TOKENS // TOK_A_DEV
    shift = jax.random.uniform(offset_random_key, (blocks, 1, ATTENTION_HEADS), jnp.float32, -0.7, 0.7)
    jitter = jax.random.uniform(noise_random_key, (blocks, TOK_A_DEV, ATTENTION_HEADS), jnp.float32, -0.5, 0.5)
    base_height = (base[None, None, :] + shift + jitter).reshape(SEQUENCE_TOKENS, ATTENTION_HEADS)
    spike_amount = jax.random.uniform(spike_random_key, (SEQUENCE_TOKENS, ATTENTION_HEADS), jnp.float32) < 8.0 / SEQUENCE_TOKENS
    spike_height = jax.random.uniform(height_random_key, (SEQUENCE_TOKENS, ATTENTION_HEADS), jnp.float32, -1.2, -0.4)
    return jnp.where(spike_amount, spike_height, base_height).astype(jnp.bfloat16)


def levels(stream_key, shape, cuts, low, largest):
    def one(axis_at, shards_of):
        heights = jax.random.uniform(jax.random.fold_in(jax.random.fold_in(stream_key, 6), axis_at), (shards_of,), jnp.float32, low / len(cuts), largest / len(cuts))
        return jnp.repeat(jnp.exp(heights), shape[axis_at] // shards_of).reshape((-1,) + (1,) * (len(shape) - axis_at - 1))

    loudness = one(*cuts[0])
    for cut in cuts[1:]:
        loudness = loudness * one(*cut)
    return loudness


def deal_out(key, own, number, rows, count, top, limit, skew):
    ranking = jax.random.permutation(key, count)
    crowded, ordinary = shares(count, rows * top, limit, skew, True), shares(count, rows * top, limit, skew, False)
    places = jnp.arange(count)

    def named(lengths, offset_by):
        used = int((lengths > 0).sum())
        fixed = max(1, used // 4)
        shifted = fixed + (places - fixed + offset_by * (used - fixed)) % max(1, count - fixed)
        return jnp.zeros((count,), jnp.int32).at[ranking[jnp.where(places < fixed, places, shifted)]].set(jnp.asarray(lengths, jnp.int32))

    lengths = jnp.where(number % 4 == 0, named(crowded, number // 4), named(ordinary, number - number // 4 - 1))
    mixed = jax.random.permutation(jax.random.fold_in(own, 3), count)
    source_of, taker = mixed[0:count // 2 * 2:2], mixed[1:count // 2 * 2:2]
    room = jnp.minimum(lengths[source_of] - 1, limit - lengths[taker]) // 2
    room = jnp.where((source_of == ranking[0]) | (taker == ranking[0]) | (lengths[taker] == 0), 0, jnp.maximum(room, 0))
    shifted = jax.random.randint(jax.random.fold_in(own, 4), (count // 2,), 0, 1 << 20) % (room + 1)
    lengths = lengths.at[source_of].add(-shifted).at[taker].add(shifted)
    items = jnp.searchsorted(jnp.cumsum(lengths), jnp.arange(rows * top), side="right").astype(jnp.int32)
    listing = items.reshape(top, rows).T
    listing = listing[jax.random.permutation(jax.random.fold_in(own, 1), rows)]
    offset_by = jax.random.randint(jax.random.fold_in(own, 2), (rows, 1), 0, top)
    return jnp.take_along_axis(listing, (jnp.arange(top)[None, :] + offset_by) % top, axis=1)


def shares(number_of, total, bound, skew, full):
    weights = [(1 << 20) // math.isqrt(standing ** skew) + 1 for standing in range(1, number_of + 1)]
    largest = bound if full else min(bound, max(-(-total // number_of), total * weights[0] // sum(weights)))
    least = 1 if total - largest >= number_of - 1 else 0
    counts, spare = [largest] + [least] * (number_of - 1), total - largest - least * (number_of - 1)
    while spare > 0:
        movable = [i for i in range(1, number_of) if counts[i] < largest] or [i for i in range(1, number_of) if counts[i] < bound]
        whole, left = sum([weights[i] for i in movable]), spare
        for i in movable:
            addition = min(bound - counts[i], max(1, left * weights[i] // whole), spare)
            counts[i] = counts[i] + addition
            spare = spare - addition
    return np.array(counts)


def bell_draw(stream_key, dims, spread, reach, cuts=(), kind=jnp.bfloat16):
    entries = jax.random.normal(stream_key, dims, jnp.float32) * spread
    if len(cuts) > 0:
        entries = levels(stream_key, dims, cuts, -0.22, 0.18) * entries
    return jnp.clip(entries, min=-reach, max=reach).astype(kind)


def setup_inputs(seed: int = 0) -> dict:
    splits = jax.random.split(jax.random.key(seed), 12)
    queries = draw_queries(jax.random.fold_in(splits[11], 71), 0)
    keys = draw_keys(jax.random.fold_in(splits[11], 71), 0)
    values = draw_values(jax.random.fold_in(splits[11], 71), 0)
    key_offset = draw_key_offset(jax.random.fold_in(splits[11], 71), 0)
    rows = bell_draw(splits[4], (TOKENS_B, D), 1.0, 6.0, ((0, 32),))
    gain = jnp.clip(1.0 + 0.18 * jax.random.normal(splits[5], (D,), jnp.float32), 0.1, 1.9)
    gate_w = bell_draw(splits[6], (EXPERTS, D, FF), D ** -0.5, 0.125, ((0, 32), (2, 16)))
    up_w = bell_draw(splits[7], (EXPERTS, D, FF), D ** -0.5, 0.125, ((0, 32), (2, 16)))
    down_w = bell_draw(splits[8], (EXPERTS, FF, D), FF ** -0.5, 0.09375, ((0, 32), (1, 16)))
    expert_ids_keys = jax.random.split(jax.random.fold_in(splits[9], 1), TOKENS_B // TOK_B_DEV)
    expert_ids_turns = jax.random.permutation(jax.random.fold_in(splits[9], 3), TOKENS_B // TOK_B_DEV)
    expert_ids = jax.vmap(lambda own, number: deal_out(jax.random.fold_in(splits[9], 2), own, number, TOK_B_DEV, EXPERTS, TOP, CAP, 0))(expert_ids_keys, expert_ids_turns).reshape((TOKENS_B, TOP))
    route_weights = jnp.clip(0.2 + 0.8 * jax.random.uniform(splits[10], (TOKENS_B, TOP), jnp.float32) ** levels(splits[10], (TOKENS_B, TOP), ((0, 32),), -0.2, 0.2), 0.2, 1.0)
    return dict(queries=queries, keys=keys, values=values, key_offset=key_offset, rows=rows, gain=gain, gate_w=gate_w, up_w=up_w, down_w=down_w, expert_ids=expert_ids, route_weights=route_weights)


EPSILON = 1e-06

def stick_mixer(queries, keys, values, key_offset):
    blocks = SEQUENCE_TOKENS // TOK_A_DEV
    scale = HD ** (-0.5)
    query_all = queries.astype(jnp.float32).reshape(blocks, TOK_A_DEV, ATTENTION_HEADS, HD)
    key_all = keys.astype(jnp.float32).reshape(blocks, TOK_A_DEV, ATTENTION_HEADS, HD)
    value_all = values.astype(jnp.float32).reshape(blocks, TOK_A_DEV, ATTENTION_HEADS, HD)
    offset_all = key_offset.astype(jnp.float32).reshape(blocks, TOK_A_DEV, ATTENTION_HEADS)
    positions = jnp.arange(TOK_A_DEV, dtype=jnp.int32)
    results = []
    for query_block in range(blocks):
        query_here = query_all[query_block]
        query_pos = query_block * TOK_A_DEV + positions

        def one_block(key_block):
            key_here = lax.dynamic_index_in_dim(key_all, key_block, 0, keepdims=False)
            value_here = lax.dynamic_index_in_dim(value_all, key_block, 0, keepdims=False)
            offset_here = lax.dynamic_index_in_dim(offset_all, key_block, 0, keepdims=False)
            logits = jnp.einsum('qhd,khd->hqk', query_here, key_here) * scale + offset_here.T[:, None, :]
            key_pos = key_block * TOK_A_DEV + positions
            strict = key_pos[None, None, :] < query_pos[None, :, None]
            breaks = jnp.where(strict, jax.nn.log_sigmoid(-logits), 0.0)
            within = lax.cumsum(breaks, axis=2, reverse=True) - breaks
            local = jnp.where(strict, jnp.exp(jax.nn.log_sigmoid(logits) + within), 0.0).astype(jnp.bfloat16)
            local = lax.optimization_barrier(local).astype(jnp.float32)
            summed = jnp.einsum('hqk,khd->hqd', local, value_here)
            return (summed, lax.optimization_barrier(jnp.sum(breaks, axis=2)))
        sums, totals = lax.map(one_block, jnp.arange(query_block + 1, dtype=jnp.int32))
        later = lax.cumsum(totals, axis=0, reverse=True) - totals
        combined = jnp.einsum('bhq,bhqd->qhd', jnp.exp(later), sums, precision=lax.Precision.HIGHEST)
        results.append(combined.reshape(TOK_A_DEV, ATTENTION_HEADS * HD))
    return jnp.concatenate(results, axis=0).astype(jnp.bfloat16)

def routed_experts(rows, gain, gate_w, up_w, down_w, expert_ids, route_weights):
    blocks = TOKENS_B // TOK_B_DEV
    rows_float = rows.astype(jnp.float32)
    normed = rows_float * lax.rsqrt(lax.optimization_barrier(jnp.mean(rows_float * rows_float, axis=1, keepdims=True)) + EPSILON)
    normed = (normed * gain.astype(jnp.float32)[None, :]).astype(jnp.bfloat16)
    block_ids = expert_ids.reshape(blocks, TOK_B_DEV * TOP)
    onehot = (block_ids[:, :, None] == jnp.arange(EXPERTS, dtype=jnp.int32)[None, None, :]).astype(jnp.int32)
    ranked = lax.optimization_barrier(jnp.sum((jnp.cumsum(onehot, axis=1) - onehot) * onehot, axis=2))
    token_of = jnp.arange(TOK_B_DEV * TOP, dtype=jnp.int32) // TOP

    def fill_table(ids_here, rank_here, block_index):
        table = jnp.zeros((EXPERTS * CAP,), jnp.int32)
        return table.at[ids_here * CAP + rank_here].set(token_of + block_index * TOK_B_DEV)
    tables = jax.vmap(fill_table)(block_ids, ranked, jnp.arange(blocks, dtype=jnp.int32))
    tables = tables.reshape(blocks, EXPERTS, CAP).transpose(1, 0, 2)
    group_width = FF // N_TP

    def one_expert(args):
        table, weight_gate, weight_up, weight_down = args
        inputs = normed[table.reshape(-1)]
        gate_val = jnp.dot(inputs, weight_gate, preferred_element_type=jnp.float32)
        up_val = jnp.dot(inputs, weight_up, preferred_element_type=jnp.float32)
        hidden = (jax.nn.silu(gate_val) * up_val).astype(jnp.bfloat16)
        grouped = hidden.reshape(-1, N_TP, group_width).astype(jnp.float32)
        down_grouped = weight_down.reshape(N_TP, group_width, D).astype(jnp.float32)
        parts = jnp.einsum('rnf,nfd->nrd', grouped, down_grouped).astype(jnp.bfloat16)
        parts = lax.optimization_barrier(parts).astype(jnp.float32)
        return lax.optimization_barrier(jnp.sum(parts, axis=0)).astype(jnp.bfloat16)
    outputs = lax.map(one_expert, (tables, gate_w, up_w, down_w))
    flat = outputs.reshape(EXPERTS * blocks * CAP, D)
    block_of = jnp.arange(TOKENS_B * TOP, dtype=jnp.int32) // (TOK_B_DEV * TOP)
    slot_index = block_ids.reshape(-1) * (blocks * CAP) + block_of * CAP + ranked.reshape(-1)
    picked = flat[slot_index].astype(jnp.float32).reshape(TOKENS_B, TOP, D)
    return lax.optimization_barrier(jnp.sum(picked * route_weights.astype(jnp.float32)[:, :, None], axis=1)).astype(jnp.bfloat16)

def reference(queries, keys, values, key_offset, rows, gain, gate_w, up_w, down_w, expert_ids, route_weights):
    attended = stick_mixer(queries, keys, values, key_offset)
    mixed = routed_experts(rows, gain, gate_w, up_w, down_w, expert_ids, route_weights)
    return (attended, mixed)
```

```python
import functools

import jax
import jax.numpy as jnp
from jax import lax
from jax.experimental import pallas as pl
from jax.experimental.pallas import tpu as pltpu
from jax.sharding import Mesh
from jax.sharding import PartitionSpec as P

EPSILON = 1e-06
LOG2E = 1.4426950408889634
F32 = jnp.float32
BF16 = jnp.bfloat16
Z, X, Y, CORE = 8, 4, 8, 2
EP = ("z", "x")
TP = ("y", "core")
LANES = 128


def dot(a, b, dims=((1,), (0,))):
    return lax.dot_general(a, b, (dims, ((), ())), preferred_element_type=F32)


def block_kernel(depth, width, len_, hd, at_ref, q_ref, kvo_ref, sums_ref, totals_ref, tri_ref, tot_ref):
    z, x = at_ref[0], at_ref[1]
    c = hd**-0.5 * LOG2E
    rows_i = lax.broadcasted_iota(jnp.int32, (len_, len_), 0)
    cols_i = lax.broadcasted_iota(jnp.int32, (len_, len_), 1)
    tri_ref[...] = jnp.where(rows_i > cols_i, -1.0, 0.0).astype(BF16)
    tot_ref[...] = jnp.zeros_like(tot_ref)
    lane = lax.broadcasted_iota(jnp.int32, (len_, LANES), 1)
    n_off = len_ // LANES

    def pair(at, a, masked):
        rows = pl.ds(pl.multiple_of(a * len_, len_), len_)
        q = q_ref[rows, :]
        k = kvo_ref[at, pl.ds(0, len_), :]
        v = kvo_ref[at, pl.ds(len_, len_), :]
        o = kvo_ref[at, pl.ds(2 * len_, 16), :].astype(F32)
        off = jnp.concatenate([o[i : i + 1, :] for i in range(n_off)], axis=1) * LOG2E
        u = dot(q, k, ((1,), (1,))) * c + off
        sp = kept = jnp.maximum(u, 0.0) + jnp.log2(1.0 + jnp.exp2(-jnp.abs(u)))
        if masked:
            strict = cols_i < rows_i
            kept = jnp.where(strict, sp, 0.0)
        w = dot(kept.astype(BF16), tri_ref[...])
        p = jnp.exp2(u - sp + w)
        if masked:
            p = jnp.where(strict, p, 0.0)
        sums_ref[at, rows, :] = dot(p.astype(BF16), v).astype(sums_ref.dtype)
        total = jnp.broadcast_to(w[:, 0:1] - kept[:, 0:1], (len_, LANES))
        tot_ref[rows, :] = jnp.where(lane == at, total, tot_ref[rows, :])

    def full(i, carry):
        early = i < width * z
        pair(
            jnp.where(early, i // width, z),
            jnp.where(early, i % width, x + 1 + i - width * z),
            False,
        )
        return carry

    lax.fori_loop(0, width * z + width - 1 - x, full, 0)
    pair(z, x, True)

    def clear(i, carry):
        early = i < x
        at = jnp.where(early, z, z + 1 + (i - x) // width)
        a = jnp.where(early, i, (i - x) % width)
        rows = pl.ds(pl.multiple_of(a * len_, len_), len_)
        sums_ref[at, rows, :] = jnp.zeros((len_, hd), sums_ref.dtype)
        return carry

    lax.fori_loop(0, x + width * (depth - 1 - z), clear, 0)
    for r in range(0, width * len_, LANES):
        totals_ref[:, r : r + LANES] = tot_ref[r : r + LANES, :].T[:depth, :]


def join_kernel(depth, width, at_ref, totals_ref, sums_ref, out_ref, scale_ref):
    z, x = at_ref[0], at_ref[1]
    later = jnp.zeros((1, totals_ref.shape[2]), F32)
    scale_ref[...] = jnp.zeros_like(scale_ref)
    for at in reversed(range(depth)):
        mine = later
        for other in range(width):
            t = totals_ref[other, at : at + 1, :]
            mine = mine + jnp.where(other > x, t, 0.0)
            later = later + t
        scale_ref[at : at + 1, :] = jnp.exp2(mine)
    for r in range(0, totals_ref.shape[2], LANES):
        cols = scale_ref[:, r : r + LANES].T
        acc = jnp.zeros((LANES, out_ref.shape[1]), F32)
        for at in range(depth):
            acc = acc + sums_ref[at, r : r + LANES, :].astype(F32) * cols[:, at : at + 1]
        out_ref[r : r + LANES, :] = acc.astype(out_ref.dtype)


def vmem(n):
    return [pl.BlockSpec(memory_space=pltpu.VMEM)] * n


SMEM = pl.BlockSpec(memory_space=pltpu.SMEM)


def stick_mixer(queries, keys, values, key_offset):
    depth, width = lax.axis_size("z"), lax.axis_size("x")
    len_, hd = queries.shape
    at = jnp.stack([lax.axis_index("z"), lax.axis_index("x")]).astype(jnp.int32)
    off = jnp.pad(key_offset.reshape(-1, LANES), ((0, 16 - len_ // LANES), (0, 0)))
    kvo = jnp.concatenate([keys, values, off], axis=0)
    kvo = lax.all_gather(kvo, "z")
    q = lax.all_gather(queries, "x", tiled=True)
    n = width * len_
    sums, totals = pl.pallas_call(
        functools.partial(block_kernel, depth, width, len_, hd),
        out_shape=(
            jax.ShapeDtypeStruct((depth, n, hd), BF16),
            jax.ShapeDtypeStruct((depth, n), F32),
        ),
        in_specs=[SMEM] + vmem(2),
        out_specs=tuple(vmem(2)),
        scratch_shapes=[pltpu.VMEM((len_, len_), BF16), pltpu.VMEM((n, LANES), F32)],
        compiler_params=pltpu.CompilerParams(vmem_limit_bytes=40 << 20),
        cost_estimate=pl.CostEstimate(
            flops=depth * n * len_ * (2 * hd + 2 * len_ + 2 * hd),
            transcendentals=3 * depth * n * len_,
            bytes_accessed=depth * n * hd * 2 + kvo.size * 2 + q.size * 2,
        ),
        name="stick_blocks",
    )(at, q, kvo)
    totals = lax.all_gather(totals, "x")
    part = pl.pallas_call(
        functools.partial(join_kernel, depth, width),
        out_shape=jax.ShapeDtypeStruct((n, hd), BF16),
        in_specs=[SMEM] + vmem(2),
        out_specs=vmem(1)[0],
        scratch_shapes=[pltpu.VMEM((LANES, n), F32)],
        cost_estimate=pl.CostEstimate(
            flops=2 * depth * n * hd, transcendentals=depth * n, bytes_accessed=depth * n * hd * 2
        ),
        name="stick_join",
    )(at, totals, sums)
    parts = lax.all_to_all(part.reshape(width, len_, hd), "x", 0, 0, tiled=True)
    return parts.astype(F32).sum(axis=0).astype(BF16)


def dispatch_kernel(cap, at_ref, rows_ref, gain_ref, ids_ref, wts_ref, out_ref, hi_ref, lo_ref):
    tok = rows_ref.shape[0]
    width = out_ref.shape[1]
    slots = out_ref.shape[0]
    rows = rows_ref[...].astype(F32)
    rms = lax.rsqrt(jnp.mean(rows * rows, axis=1, keepdims=True) + EPSILON)
    own = pl.ds(pl.multiple_of(at_ref[0] * width, width), width)
    normed = (rows_ref[:, own].astype(F32) * rms * gain_ref[:, own]).astype(BF16)
    first, second = ids_ref[:, 0:1], ids_ref[:, 1:2]
    lane = lax.broadcasted_iota(jnp.int32, (tok, LANES), 1)
    chosen = jnp.where((first == lane) | (second == lane), 1.0, 0.0).astype(BF16)
    before = lax.broadcasted_iota(jnp.int32, (tok, tok), 1) < lax.broadcasted_iota(
        jnp.int32, (tok, tok), 0
    )
    rank = dot(jnp.where(before, 1.0, 0.0).astype(BF16), chosen).astype(BF16)
    spread = (
        lax.broadcasted_iota(jnp.int32, (LANES, slots), 1) // cap
        == lax.broadcasted_iota(jnp.int32, (LANES, slots), 0)
    )
    spread = jnp.where(spread, 1.0, 0.0).astype(BF16)
    slot = lax.broadcasted_iota(jnp.int32, (tok, slots), 1)
    taken = (dot(chosen, spread) > 0.5) & (dot(rank, spread) == (slot % cap).astype(F32))
    pick = jnp.where(taken, 1.0, 0.0).astype(BF16)
    out_ref[...] = dot(pick, normed, ((0,), (0,))).astype(BF16)
    weight = jnp.where(slot // cap == first, wts_ref[:, 0:1], wts_ref[:, 1:2])
    weight = jnp.where(taken, weight, 0.0)
    hi = weight.astype(BF16)
    hi_ref[...] = hi
    lo_ref[...] = (weight - hi.astype(F32)).astype(BF16)


def routed_experts(rows, gain, gate_w, up_w, down_w, expert_ids, route_weights):
    experts = lax.axis_size(EP)
    groups = lax.axis_size(TP)
    tok, width = rows.shape
    own = width // groups
    cap = 2 * expert_ids.shape[1] * tok // experts
    slots = experts * cap
    at = jnp.stack([lax.axis_index(TP)]).astype(jnp.int32)
    outgoing, hi, lo = pl.pallas_call(
        functools.partial(dispatch_kernel, cap),
        out_shape=(
            jax.ShapeDtypeStruct((slots, own), BF16),
            jax.ShapeDtypeStruct((tok, slots), BF16),
            jax.ShapeDtypeStruct((tok, slots), BF16),
        ),
        in_specs=[SMEM] + vmem(4),
        out_specs=tuple(vmem(3)),
        name="dispatch",
    )(at, rows, gain.reshape(1, -1), expert_ids, route_weights)
    arrived = lax.all_to_all(outgoing.reshape(experts, cap, own), EP, 0, 0, tiled=True)
    arrived = lax.all_gather(arrived.reshape(slots, own), TP)
    gate = jnp.einsum(
        "jsc,jcf->sf", arrived, gate_w.reshape(groups, own, -1), preferred_element_type=F32
    )
    up = jnp.einsum(
        "jsc,jcf->sf", arrived, up_w.reshape(groups, own, -1), preferred_element_type=F32
    )
    hidden = (jax.nn.silu(gate) * up).astype(BF16)
    part = jnp.einsum(
        "sf,fjc->jsc", hidden, down_w.reshape(-1, groups, own), preferred_element_type=F32
    ).astype(BF16)
    share = lax.psum_scatter(part, TP, scatter_dimension=0, tiled=True)
    back = lax.all_to_all(share.reshape(experts, cap, own), EP, 0, 0, tiled=True)
    back = back.reshape(slots, own)
    mixed = (dot(hi, back) + dot(lo, back)).astype(BF16)
    return lax.all_gather(mixed, TP, axis=1, tiled=True)


def body(
    queries, keys, values, key_offset, rows, gain, gate_w, up_w, down_w, expert_ids, route_weights
):
    mixed = routed_experts(rows, gain, gate_w, up_w, down_w, expert_ids, route_weights)
    attended = stick_mixer(queries, keys, values, key_offset)
    return (attended, mixed)


def solution(mesh):
    fine = Mesh(mesh.devices.reshape(Z, X, Y, CORE), ("z", "x", "y", "core"))
    return jax.shard_map(
        body,
        mesh=fine,
        in_specs=(
            P(EP, TP),
            P(EP, TP),
            P(EP, TP),
            P(EP, TP),
            P(EP, None),
            P(),
            P(EP, None, TP),
            P(EP, None, TP),
            P(EP, TP, None),
            P(EP, None),
            P(EP, None),
        ),
        out_specs=(P(EP, TP), P(EP, None)),
        check_vma=False,
    )
```

```python
import functools

import jax
import jax.numpy as jnp
from jax import lax
from jax.experimental import pallas as pl
from jax.experimental.pallas import tpu as pltpu
from jax.sharding import Mesh
from jax.sharding import PartitionSpec as P

EPSILON = 1e-06
LOG2E = 1.4426950408889634
F32 = jnp.float32
BF16 = jnp.bfloat16
Z, X, Y, CORE = 8, 4, 8, 2
EP = ("z", "x")
TP = ("y", "core")
LANES = 128


def dot(a, b, dims=((1,), (0,))):
    return lax.dot_general(a, b, (dims, ((), ())), preferred_element_type=F32)


def block_kernel(depth, width, len_, hd, at_ref, q_ref, kvo_ref, out_ref, tri_ref, tot_ref, acc_ref, carry_ref):
    z, x = at_ref[0], at_ref[1]
    c = hd**-0.5 * LOG2E
    rows_i = lax.broadcasted_iota(jnp.int32, (len_, len_), 0)
    cols_i = lax.broadcasted_iota(jnp.int32, (len_, len_), 1)
    tri_ref[...] = jnp.where(rows_i > cols_i, -1.0, 0.0).astype(BF16)
    tot_ref[...] = jnp.zeros_like(tot_ref)
    lane = lax.broadcasted_iota(jnp.int32, (len_, LANES), 1)
    n_off = len_ // LANES

    def pair(to, k_at, old, masked):
        q = q_ref[to]
        k = kvo_ref[k_at, pl.ds(0, len_), :]
        v = kvo_ref[k_at, pl.ds(len_, len_), :]
        o = kvo_ref[k_at, pl.ds(2 * len_, 16), :].astype(F32)
        off = jnp.concatenate([o[i : i + 1, :] for i in range(n_off)], axis=1) * LOG2E
        u = dot(q, k, ((1,), (1,))) * c + off
        sp = kept = jnp.maximum(u, 0.0) + jnp.log2(1.0 + jnp.exp2(-jnp.abs(u)))
        if masked:
            strict = cols_i < rows_i
            kept = jnp.where(strict, sp, 0.0)
        w = dot(kept.astype(BF16), tri_ref[...])
        p = jnp.exp2(u - sp + w)
        if masked:
            p = jnp.where(strict, p, 0.0)
        total = jnp.broadcast_to(w[:, 0:1] - kept[:, 0:1], (len_, LANES))
        summed = dot(p.astype(BF16), v)
        if masked:
            acc, carry = summed, total
        else:
            carry = carry_ref[...] * old
            acc = acc_ref[...] * old + jnp.exp2(carry) * summed
            carry = carry + total
        carry_ref[...] = carry
        acc_ref[...] = acc
        out_ref[to, pl.ds(0, len_), :] = acc.astype(BF16)
        tot_ref[...] = jnp.where(lane == to, carry, tot_ref[...])

    pair(z, x, None, True)

    def full(i, done):
        own = i < x
        j = i - x
        fresh = jnp.logical_and(jnp.logical_not(own), j % width == 0)
        pair(
            jnp.where(own, z, z + 1 + j // width),
            jnp.where(own, x - 1 - i, width - 1 - j % width),
            jnp.where(fresh, 0.0, 1.0),
            False,
        )
        return done

    lax.fori_loop(0, x + width * (depth - 1 - z), full, 0)

    def clear(i, done):
        out_ref[i, pl.ds(0, len_), :] = jnp.zeros((len_, hd), BF16)
        return done

    lax.fori_loop(0, z, clear, 0)
    cols = [tot_ref[r * LANES : (r + 1) * LANES, :].T for r in range(n_off)]
    for to in range(depth):
        rest = [col[to : to + 1, :] for col in cols]
        terms = []
        for _ in range(3):
            term = [r.astype(BF16).astype(F32) for r in rest]
            rest = [r - t for r, t in zip(rest, term)]
            terms += term
        terms.append(jnp.zeros((16 - len(terms), LANES), F32))
        out_ref[to, pl.ds(len_, 16), :] = jnp.concatenate(terms, axis=0).astype(BF16)


def join_kernel(depth, len_, in_ref, out_ref, scale_ref):
    n_off = len_ // LANES
    later = [jnp.zeros((1, LANES), F32)] * n_off
    scale_ref[...] = jnp.zeros_like(scale_ref)
    for at in reversed(range(depth)):
        t = in_ref[at, pl.ds(len_, 16), :].astype(F32)
        for r in range(n_off):
            scale_ref[at : at + 1, r * LANES : (r + 1) * LANES] = jnp.exp2(later[r])
            for term in range(3):
                i = term * n_off + r
                later[r] = later[r] + t[i : i + 1, :]
    for r in range(n_off):
        rows = slice(r * LANES, (r + 1) * LANES)
        cols = scale_ref[:, rows].T
        acc = jnp.zeros((LANES, out_ref.shape[1]), F32)
        for at in range(depth):
            acc = acc + in_ref[at, rows, :].astype(F32) * cols[:, at : at + 1]
        out_ref[rows, :] = acc.astype(out_ref.dtype)


def vmem(n):
    return [pl.BlockSpec(memory_space=pltpu.VMEM)] * n


SMEM = pl.BlockSpec(memory_space=pltpu.SMEM)


def stick_mixer(queries, keys, values, key_offset):
    depth, width = lax.axis_size("z"), lax.axis_size("x")
    len_, hd = queries.shape
    at = jnp.stack([lax.axis_index("z"), lax.axis_index("x")]).astype(jnp.int32)
    off = jnp.pad(key_offset.reshape(-1, LANES), ((0, 16 - len_ // LANES), (0, 0)))
    kvo = jnp.concatenate([keys, values, off], axis=0)
    kvo = lax.all_gather(kvo, "x")
    q = lax.all_gather(queries, "z")
    sums = pl.pallas_call(
        functools.partial(block_kernel, depth, width, len_, hd),
        out_shape=jax.ShapeDtypeStruct((depth, len_ + 16, hd), BF16),
        in_specs=[SMEM] + vmem(2),
        out_specs=vmem(1)[0],
        scratch_shapes=[
            pltpu.VMEM((len_, len_), BF16),
            pltpu.VMEM((len_, LANES), F32),
            pltpu.VMEM((len_, hd), F32),
            pltpu.VMEM((len_, LANES), F32),
        ],
        compiler_params=pltpu.CompilerParams(vmem_limit_bytes=32 << 20),
        cost_estimate=pl.CostEstimate(
            flops=depth * width * len_ * len_ * (4 * hd + 2 * len_),
            transcendentals=3 * depth * width * len_ * len_,
            bytes_accessed=2 * (2 * depth * len_ * hd + kvo.size),
        ),
        name="stick_blocks",
    )(at, q, kvo)
    sums = lax.all_to_all(sums, "z", 0, 0, tiled=True)
    return pl.pallas_call(
        functools.partial(join_kernel, depth, len_),
        out_shape=jax.ShapeDtypeStruct((len_, hd), BF16),
        in_specs=vmem(1),
        out_specs=vmem(1)[0],
        scratch_shapes=[pltpu.VMEM((LANES, len_), F32)],
        cost_estimate=pl.CostEstimate(
            flops=2 * depth * len_ * hd, transcendentals=depth * len_, bytes_accessed=2 * depth * len_ * hd
        ),
        name="stick_join",
    )(sums)


def dispatch_kernel(cap, at_ref, rows_ref, gain_ref, ids_ref, wts_ref, out_ref, hi_ref, lo_ref):
    tok, slots = rows_ref.shape[0], out_ref.shape[0]
    rows = rows_ref[...].astype(F32)
    rms = lax.rsqrt(jnp.mean(rows * rows, axis=1, keepdims=True) + EPSILON)
    first, second = ids_ref[:, 0:1], ids_ref[:, 1:2]
    lane = lax.broadcasted_iota(jnp.int32, (tok, LANES), 1)
    chosen = jnp.where((first == lane) | (second == lane), 1.0, 0.0).astype(BF16)
    before = lax.broadcasted_iota(jnp.int32, (tok, tok), 1) < lax.broadcasted_iota(
        jnp.int32, (tok, tok), 0
    )
    rank = dot(jnp.where(before, 1.0, 0.0).astype(BF16), chosen).astype(BF16)
    spread = (
        lax.broadcasted_iota(jnp.int32, (LANES, slots), 1) // cap
        == lax.broadcasted_iota(jnp.int32, (LANES, slots), 0)
    )
    spread = jnp.where(spread, 1.0, 0.0).astype(BF16)
    slot = lax.broadcasted_iota(jnp.int32, (tok, slots), 1)
    taken = (dot(chosen, spread) > 0.5) & (dot(rank, spread) == (slot % cap).astype(F32))
    pick = jnp.where(taken, 1.0, 0.0).astype(BF16)
    for i in range(out_ref.shape[1] // LANES):
        own = pl.ds(pl.multiple_of((2 * i + at_ref[0]) * LANES, LANES), LANES)
        normed = (rows_ref[:, own].astype(F32) * rms * gain_ref[:, own]).astype(BF16)
        out_ref[:, i * LANES : (i + 1) * LANES] = dot(pick, normed, ((0,), (0,))).astype(BF16)
    weight = jnp.where(slot // cap == first, wts_ref[:, 0:1], wts_ref[:, 1:2])
    weight = jnp.where(taken, weight, 0.0)
    hi = weight.astype(BF16)
    hi_ref[...] = hi
    lo_ref[...] = (weight - hi.astype(F32)).astype(BF16)


def expert_kernel(at_ref, mine_ref, other_ref, gate_ref, up_ref, down_ref, keep_ref, send_ref, all_ref):
    core = at_ref[0]
    chunks = mine_ref.shape[1] // LANES
    for i in range(chunks):
        here = slice(i * LANES, (i + 1) * LANES)
        all_ref[:, pl.ds(pl.multiple_of((2 * i + core) * LANES, LANES), LANES)] = mine_ref[:, here]
        all_ref[:, pl.ds(pl.multiple_of((2 * i + 1 - core) * LANES, LANES), LANES)] = other_ref[:, here]
    tokens = all_ref[...]
    gate = dot(tokens, gate_ref[...], ((1,), (1,)))
    up = dot(tokens, up_ref[...], ((1,), (1,)))
    hidden = (gate / (1.0 + jnp.exp(-gate)) * up).astype(BF16)
    all_ref[...] = dot(hidden, down_ref[...]).astype(BF16)
    for i in range(chunks):
        here = slice(i * LANES, (i + 1) * LANES)
        keep_ref[:, here] = all_ref[:, pl.ds(pl.multiple_of((2 * i + core) * LANES, LANES), LANES)]
        send_ref[:, here] = all_ref[:, pl.ds(pl.multiple_of((2 * i + 1 - core) * LANES, LANES), LANES)]


def swap(x):
    return lax.ppermute(x, "core", [(0, 1), (1, 0)])


def routed_experts(rows, gain, gate_w, up_w, down_w, expert_ids, route_weights):
    experts = lax.axis_size(EP)
    tok, width = rows.shape
    half = width // lax.axis_size("core")
    hosts = lax.axis_size("y")
    cap = 2 * expert_ids.shape[1] * tok // experts
    slots = experts * cap
    at = jnp.stack([lax.axis_index("core")]).astype(jnp.int32)
    outgoing, hi, lo = pl.pallas_call(
        functools.partial(dispatch_kernel, cap),
        out_shape=(
            jax.ShapeDtypeStruct((slots, half), BF16),
            jax.ShapeDtypeStruct((tok, slots), BF16),
            jax.ShapeDtypeStruct((tok, slots), BF16),
        ),
        in_specs=[SMEM] + vmem(4),
        out_specs=tuple(vmem(3)),
        name="dispatch",
    )(at, rows, gain.reshape(1, -1), expert_ids, route_weights)
    mine = lax.all_to_all(outgoing.reshape(experts, cap, half), EP, 0, 0, tiled=True)
    mine = mine.reshape(slots, half)
    hidden = gate_w.shape[2]
    keep, send = pl.pallas_call(
        expert_kernel,
        out_shape=(jax.ShapeDtypeStruct((slots, half), BF16),) * 2,
        in_specs=[SMEM] + vmem(5),
        out_specs=tuple(vmem(2)),
        scratch_shapes=[pltpu.VMEM((slots, width), BF16)],
        compiler_params=pltpu.CompilerParams(vmem_limit_bytes=32 << 20),
        cost_estimate=pl.CostEstimate(
            flops=6 * slots * width * hidden,
            transcendentals=slots * hidden,
            bytes_accessed=2 * (2 * slots * width + 3 * width * hidden),
        ),
        name="experts",
    )(at, mine, swap(mine), gate_w[0].T, up_w[0].T, down_w[0])
    share = (keep.astype(F32) + swap(send).astype(F32)).astype(BF16)
    back = lax.all_to_all(share.reshape(experts, cap, half), EP, 0, 0, tiled=True)
    back = back.reshape(slots, half)
    partial = (dot(hi, back) + dot(lo, back)).astype(BF16)
    partial = jnp.moveaxis(partial.reshape(tok, hosts, -1), 1, 0)
    partial = lax.all_to_all(partial, "y", 0, 0, tiled=True)
    mixed = partial.astype(F32).sum(axis=0).astype(BF16)
    return lax.all_gather(mixed, TP, axis=1, tiled=True)


def body(
    queries, keys, values, key_offset, rows, gain, gate_w, up_w, down_w, expert_ids, route_weights
):
    mixed = routed_experts(rows, gain, gate_w, up_w, down_w, expert_ids, route_weights)
    attended = stick_mixer(queries, keys, values, key_offset)
    return (attended, mixed)


def solution(mesh):
    fine = Mesh(mesh.devices.reshape(Z, X, Y, CORE), ("z", "x", "y", "core"))
    return jax.shard_map(
        body,
        mesh=fine,
        in_specs=(
            P(EP, TP),
            P(EP, TP),
            P(EP, TP),
            P(EP, TP),
            P(EP, None),
            P(),
            P(EP, None, TP),
            P(EP, None, TP),
            P(EP, TP, None),
            P(EP, None),
            P(EP, None),
        ),
        out_specs=(P(EP, TP), P(EP, None)),
        check_vma=False,
    )
```

```python
import functools

import jax
import jax.numpy as jnp
from jax import lax
from jax.experimental import pallas as pl
from jax.experimental.pallas import tpu as pltpu
from jax.sharding import Mesh
from jax.sharding import PartitionSpec as P


EPSILON = 1e-06
LOG2E = 1.4426950408889634
F32 = jnp.float32
BF16 = jnp.bfloat16
EXTRA1 = 0
EXTRA2 = 0
Z, X, Y, CORE = 8, 4, 8, 2
EP = ("z", "x")
TP = ("y", "core")
LANES = 128


def dot(a, b, dims=((1,), (0,))):
    return lax.dot_general(a, b, (dims, ((), ())), preferred_element_type=F32)


def block_kernel(depth, width, len_, hd, at_ref, q_ref, *refs):
    near, (out_ref, kvo_ref, tri_ref, tot_ref, acc_ref, carry_ref) = refs[:width], refs[width:]
    z, x = at_ref[0], at_ref[1]
    for step in range(width):
        kvo_ref[(x + width - step) % width] = near[step][...]
    c = hd**-0.5 * LOG2E
    rows_i = lax.broadcasted_iota(jnp.int32, (len_, len_), 0)
    cols_i = lax.broadcasted_iota(jnp.int32, (len_, len_), 1)
    tri_ref[...] = jnp.where(rows_i > cols_i, -1.0, 0.0).astype(BF16)
    tot_ref[...] = jnp.zeros_like(tot_ref)
    lane = lax.broadcasted_iota(jnp.int32, (len_, LANES), 1)
    n_off = len_ // LANES

    def pair(to, k_at, old, masked):
        q = q_ref[to]
        k = kvo_ref[k_at, pl.ds(0, len_), :]
        v = kvo_ref[k_at, pl.ds(len_, len_), :]
        o = kvo_ref[k_at, pl.ds(2 * len_, 16), :].astype(F32)
        off = jnp.concatenate([o[i : i + 1, :] for i in range(n_off)], axis=1) * LOG2E
        u = dot(q, k, ((1,), (1,))) * c + off
        sp = kept = jnp.maximum(u, 0.0) + jnp.log2(1.0 + jnp.exp2(-jnp.abs(u)))
        if masked:
            strict = cols_i < rows_i
            kept = jnp.where(strict, sp, 0.0)
        w = dot(kept.astype(BF16), tri_ref[...])
        p = jnp.exp2(u - sp + w)
        if masked:
            p = jnp.where(strict, p, 0.0)
        total = jnp.broadcast_to(w[:, 0:1] - kept[:, 0:1], (len_, LANES))
        summed = dot(p.astype(BF16), v)
        if masked:
            acc, carry = summed, total
        else:
            carry = carry_ref[...] * old
            acc = acc_ref[...] * old + jnp.exp2(carry) * summed
            carry = carry + total
        carry_ref[...] = carry
        acc_ref[...] = acc
        out_ref[to, pl.ds(0, len_), :] = acc.astype(BF16)
        tot_ref[...] = jnp.where(lane == to, carry, tot_ref[...])

    pair(z, x, None, True)

    def full(i, done):
        own = i < x
        j = i - x
        fresh = jnp.logical_and(jnp.logical_not(own), j % width == 0)
        pair(
            jnp.where(own, z, z + 1 + j // width),
            jnp.where(own, x - 1 - i, width - 1 - j % width),
            jnp.where(fresh, 0.0, 1.0),
            False,
        )
        return done

    lax.fori_loop(0, x + width * (depth - 1 - z), full, 0)

    def clear(i, done):
        out_ref[i, pl.ds(0, len_), :] = jnp.zeros((len_, hd), BF16)
        return done

    lax.fori_loop(0, z, clear, 0)
    cols = [tot_ref[r * LANES : (r + 1) * LANES, :].T for r in range(n_off)]
    for to in range(depth):
        rest = [col[to : to + 1, :] for col in cols]
        terms = []
        for _ in range(3):
            term = [r.astype(BF16).astype(F32) for r in rest]
            rest = [r - t for r, t in zip(rest, term)]
            terms += term
        terms.append(jnp.zeros((16 - len(terms), LANES), F32))
        out_ref[to, pl.ds(len_, 16), :] = jnp.concatenate(terms, axis=0).astype(BF16)


def join_kernel(depth, len_, in_ref, out_ref, scale_ref):
    n_off = len_ // LANES
    later = [jnp.zeros((1, LANES), F32)] * n_off
    scale_ref[...] = jnp.zeros_like(scale_ref)
    for at in reversed(range(depth)):
        t = in_ref[at, pl.ds(len_, 16), :].astype(F32)
        for r in range(n_off):
            scale_ref[at : at + 1, r * LANES : (r + 1) * LANES] = jnp.exp2(later[r])
            for term in range(3):
                i = term * n_off + r
                later[r] = later[r] + t[i : i + 1, :]
    for r in range(n_off):
        rows = slice(r * LANES, (r + 1) * LANES)
        cols = scale_ref[:, rows].T
        acc = jnp.zeros((LANES, out_ref.shape[1]), F32)
        for at in range(depth):
            acc = acc + in_ref[at, rows, :].astype(F32) * cols[:, at : at + 1]
        out_ref[rows, :] = acc.astype(out_ref.dtype)


def vmem(n):
    return [pl.BlockSpec(memory_space=pltpu.VMEM)] * n


SMEM = pl.BlockSpec(memory_space=pltpu.SMEM)


def dispatch_kernel(cap, at_ref, rows_ref, gain_ref, ids_ref, wts_ref, out_ref, hi_ref, lo_ref):
    tok, slots = rows_ref.shape[0], out_ref.shape[0]
    rows = rows_ref[...].astype(F32)
    rms = lax.rsqrt(jnp.mean(rows * rows, axis=1, keepdims=True) + EPSILON)
    first, second = ids_ref[0:1, :], ids_ref[1:2, :]
    expert = lax.broadcasted_iota(jnp.int32, (LANES, tok), 0)
    chosen = jnp.where((first == expert) | (second == expert), 1.0, 0.0).astype(BF16)
    before = lax.broadcasted_iota(jnp.int32, (tok, tok), 0) < lax.broadcasted_iota(
        jnp.int32, (tok, tok), 1
    )
    rank = dot(chosen, jnp.where(before, 1.0, 0.0).astype(BF16)).astype(BF16)
    spread = (
        lax.broadcasted_iota(jnp.int32, (slots, LANES), 0) // cap
        == lax.broadcasted_iota(jnp.int32, (slots, LANES), 1)
    )
    spread = jnp.where(spread, 1.0, 0.0).astype(BF16)
    slot = lax.broadcasted_iota(jnp.int32, (slots, tok), 0)
    taken = (dot(spread, chosen) > 0.5) & (dot(spread, rank) == (slot % cap).astype(F32))
    pick = jnp.where(taken, 1.0, 0.0).astype(BF16)
    for i in range(out_ref.shape[1] // LANES):
        own = pl.ds(pl.multiple_of((2 * i + at_ref[0]) * LANES, LANES), LANES)
        normed = (rows_ref[:, own].astype(F32) * rms * gain_ref[:, own]).astype(BF16)
        out_ref[:, i * LANES : (i + 1) * LANES] = dot(pick, normed).astype(BF16)
    weight = jnp.where(slot // cap == first, wts_ref[0:1, :], wts_ref[1:2, :])
    weight = jnp.where(taken, weight, 0.0)
    hi = weight.astype(BF16)
    hi_ref[...] = hi
    lo_ref[...] = (weight - hi.astype(F32)).astype(BF16)


def expert_kernel(at_ref, mine_ref, other_ref, gate_ref, up_ref, down_ref, *rest):
    keep_ref, send_ref, all_ref = rest[-3:]
    core = at_ref[0]
    chunks = mine_ref.shape[1] // LANES
    for i in range(chunks):
        here = slice(i * LANES, (i + 1) * LANES)
        all_ref[:, pl.ds(pl.multiple_of((2 * i + core) * LANES, LANES), LANES)] = mine_ref[:, here]
        all_ref[:, pl.ds(pl.multiple_of((2 * i + 1 - core) * LANES, LANES), LANES)] = other_ref[:, here]
    tokens = all_ref[...]
    gate = dot(tokens, gate_ref[...], ((1,), (1,)))
    up = dot(tokens, up_ref[...], ((1,), (1,)))
    hidden = (gate / (1.0 + jnp.exp(-gate)) * up).astype(BF16)
    all_ref[...] = dot(hidden, down_ref[...]).astype(BF16)
    for i in range(chunks):
        keep_ref[i] = all_ref[:, pl.ds(pl.multiple_of((2 * i + core) * LANES, LANES), LANES)]
        send_ref[i] = all_ref[:, pl.ds(pl.multiple_of((2 * i + 1 - core) * LANES, LANES), LANES)]


def sum_kernel(in_ref, *rest):
    out_ref = rest[-1]
    total = in_ref[0].astype(F32)
    for i in range(1, in_ref.shape[0]):
        total = total + in_ref[i].astype(F32)
    out_ref[...] = total.astype(out_ref.dtype)


def combine_kernel(hi_ref, lo_ref, back_ref, out_ref):
    back = back_ref[...]
    out_ref[...] = (
        dot(hi_ref[...], back, ((0,), (0,))) + dot(lo_ref[...], back, ((0,), (0,)))
    ).astype(BF16)


def swap(x):
    return lax.ppermute(x, "core", [(0, 1), (1, 0)])


ANY = pl.BlockSpec(memory_space=pl.ANY)


def layer(
    queries, keys, values, key_offset, rows, gain, gate_w, up_w, down_w, expert_ids, route_weights
):
    experts = lax.axis_size(EP)
    tok, width = rows.shape
    half = width // lax.axis_size("core")
    hosts = lax.axis_size("y")
    cap = 2 * expert_ids.shape[1] * tok // experts
    slots = experts * cap
    depth, wide = lax.axis_size("z"), lax.axis_size("x")
    len_, hd = queries.shape
    core = jnp.stack([lax.axis_index("core")]).astype(jnp.int32)
    place = jnp.stack([lax.axis_index("z"), lax.axis_index("x")]).astype(jnp.int32)
    outgoing, hi, lo = pl.pallas_call(
        functools.partial(dispatch_kernel, cap),
        out_shape=(
            jax.ShapeDtypeStruct((slots, half), BF16),
            jax.ShapeDtypeStruct((slots, tok), BF16),
            jax.ShapeDtypeStruct((slots, tok), BF16),
        ),
        in_specs=[SMEM] + vmem(4),
        out_specs=tuple(vmem(3)),
        name="dispatch",
    )(core, rows, gain.reshape(1, -1), expert_ids.T, route_weights.T)
    mine = lax.all_to_all(outgoing.reshape(experts, cap, half), EP, 0, 0, tiled=True)
    mine = mine.reshape(slots, half)

    off = jnp.pad(key_offset.reshape(-1, LANES), ((0, 16 - len_ // LANES), (0, 0)))
    kvo = [jnp.concatenate([keys, values, off], axis=0)]
    for step in range(1, wide):
        kvo.append(lax.ppermute(kvo[0], "x", [(i, (i + step) % wide) for i in range(wide)]))
    q = lax.all_gather(queries, "z")

    hidden = gate_w.shape[2]
    other = swap(mine)
    keep, send = pl.pallas_call(
        expert_kernel,
        out_shape=(jax.ShapeDtypeStruct((hosts, slots, LANES), BF16),) * 2,
        in_specs=[SMEM] + vmem(5) + [ANY] * EXTRA1,
        out_specs=tuple(vmem(2)),
        scratch_shapes=[pltpu.VMEM((slots, width), BF16)],
        compiler_params=pltpu.CompilerParams(vmem_limit_bytes=32 << 20),
        cost_estimate=pl.CostEstimate(
            flops=6 * slots * width * hidden,
            transcendentals=slots * hidden,
            bytes_accessed=2 * (2 * slots * width + 3 * width * hidden),
        ),
        name="experts",
    )(core, mine, other, gate_w[0].T, up_w[0].T, down_w[0], *([q] * EXTRA1))
    other = swap(send)
    share = (keep.astype(F32) + other.astype(F32)).astype(BF16)
    share = lax.all_to_all(share, "y", 0, 0, tiled=True)

    sums = pl.pallas_call(
        functools.partial(block_kernel, depth, wide, len_, hd),
        out_shape=jax.ShapeDtypeStruct((depth, len_ + 16, hd), BF16),
        in_specs=[SMEM] + vmem(1 + wide),
        out_specs=vmem(1)[0],
        scratch_shapes=[
            pltpu.VMEM((wide, 2 * len_ + 16, hd), BF16),
            pltpu.VMEM((len_, len_), BF16),
            pltpu.VMEM((len_, LANES), F32),
            pltpu.VMEM((len_, hd), F32),
            pltpu.VMEM((len_, LANES), F32),
        ],
        compiler_params=pltpu.CompilerParams(vmem_limit_bytes=32 << 20),
        cost_estimate=pl.CostEstimate(
            flops=depth * wide * len_ * len_ * (4 * hd + 2 * len_),
            transcendentals=3 * depth * wide * len_ * len_,
            bytes_accessed=2 * (2 * depth * len_ * hd + wide * kvo[0].size),
        ),
        name="stick_blocks",
    )(place, q, *kvo)
    arrived = lax.all_to_all(sums, "z", 0, 0, tiled=True)
    attended = pl.pallas_call(
        functools.partial(join_kernel, depth, len_),
        out_shape=jax.ShapeDtypeStruct((len_, hd), BF16),
        in_specs=vmem(1),
        out_specs=vmem(1)[0],
        scratch_shapes=[pltpu.VMEM((LANES, len_), F32)],
        cost_estimate=pl.CostEstimate(
            flops=2 * depth * len_ * hd, transcendentals=depth * len_, bytes_accessed=2 * depth * len_ * hd
        ),
        name="stick_join",
    )(arrived)

    share = pl.pallas_call(
        sum_kernel,
        out_shape=jax.ShapeDtypeStruct((slots, LANES), BF16),
        in_specs=vmem(1) + [ANY] * EXTRA2,
        out_specs=vmem(1)[0],
        name="parts_sum",
    )(share, *([sums] * EXTRA2))
    back = lax.all_to_all(share.reshape(experts, cap, LANES), EP, 0, 0, tiled=True)
    mixed = pl.pallas_call(
        combine_kernel,
        out_shape=jax.ShapeDtypeStruct((tok, LANES), BF16),
        in_specs=vmem(3),
        out_specs=vmem(1)[0],
        name="combine",
    )(hi, lo, back.reshape(slots, LANES))
    mixed = lax.all_gather(mixed, TP, axis=1, tiled=True)
    return (attended, mixed)


def solution(mesh):
    fine = Mesh(mesh.devices.reshape(Z, X, Y, CORE), ("z", "x", "y", "core"))
    return jax.shard_map(
        layer,
        mesh=fine,
        in_specs=(
            P(EP, TP),
            P(EP, TP),
            P(EP, TP),
            P(EP, TP),
            P(EP, None),
            P(),
            P(EP, None, TP),
            P(EP, None, TP),
            P(EP, TP, None),
            P(EP, None),
            P(EP, None),
        ),
        out_specs=(P(EP, TP), P(EP, None)),
        check_vma=False,
    )
```

```python
import functools

import jax
import jax.numpy as jnp
from jax import lax
from jax.experimental import pallas as pl
from jax.experimental.pallas import tpu as pltpu
from jax.sharding import Mesh
from jax.sharding import PartitionSpec as P


EPSILON = 1e-06
LOG2E = 1.4426950408889634
F32 = jnp.float32
BF16 = jnp.bfloat16
Z, X, Y, CORE = 8, 4, 8, 2
EP = ("z", "x")
TP = ("y", "core")
LANES = 128
TILE = 256


def dot(a, b, dims=((1,), (0,))):
    return lax.dot_general(a, b, (dims, ((), ())), preferred_element_type=F32)


def block_kernel(depth, width, len_, hd, at_ref, q_ref, *refs):
    near, (out_ref, qq_ref, kk_ref, v_ref, off_ref, tri_ref, tot_ref, acc_ref, carry_ref) = (
        refs[:width],
        refs[width:],
    )
    z, x = at_ref[0], at_ref[1]
    n_off = len_ // LANES
    half = width * len_ // 2
    for step in range(width):
        rows = pl.ds(pl.multiple_of((x + width - step) % width * len_, len_), len_)
        for twice in range(2):
            kk_ref[rows, twice * hd : (twice + 1) * hd] = near[step][:len_, :]
        v_ref[rows, :] = near[step][len_ : 2 * len_, :]
        o = near[step][2 * len_ :, :].astype(F32) * LOG2E
        for i in range(n_off):
            at = pl.ds(pl.multiple_of(((x + width - step) % width * n_off + i) * LANES, LANES), LANES)
            off_ref[0:1, at] = o[i : i + 1, :]

    def scale(i, done):
        q = q_ref[i].astype(F32) * (hd**-0.5 * LOG2E)
        hi = q.astype(BF16)
        qq_ref[i, :, :hd] = hi
        qq_ref[i, :, hd:] = (q - hi.astype(F32)).astype(BF16)
        return done

    lax.fori_loop(z, depth, scale, 0)
    tri_ref[...] = jnp.where(
        lax.broadcasted_iota(jnp.int32, (TILE, TILE), 0) > lax.broadcasted_iota(jnp.int32, (TILE, TILE), 1),
        -1.0,
        0.0,
    ).astype(BF16)
    tot_ref[...] = jnp.zeros_like(tot_ref)
    lane = lax.broadcasted_iota(jnp.int32, (len_, LANES), 1)

    def part(to, which, old, masked):
        start = pl.multiple_of(which * half, half)
        q = qq_ref[to]
        carry = 0.0 if masked else carry_ref[...] * old
        acc = 0.0 if masked else acc_ref[...] * old
        for tile in reversed(range(half // TILE)):
            keys = pl.ds(pl.multiple_of(start + tile * TILE, TILE), TILE)
            u = dot(q, kk_ref[keys, :], ((1,), (1,))) + off_ref[0:1, keys]
            sp = kept = jnp.maximum(u, 0.0) + jnp.log2(1.0 + jnp.exp2(-jnp.abs(u)))
            if masked:
                ahead = lax.broadcasted_iota(jnp.int32, (len_, TILE), 0) - lax.broadcasted_iota(
                    jnp.int32, (len_, TILE), 1
                )
                strict = ahead > start + tile * TILE - x * len_
                kept = jnp.where(strict, sp, 0.0)
            w = dot(kept.astype(BF16), tri_ref[...])
            if isinstance(carry, float):
                p = jnp.exp2(u - sp + w)
            else:
                p = jnp.exp2(u - sp + w + jnp.concatenate([carry] * (TILE // LANES), axis=1))
            if masked:
                p = jnp.where(strict, p, 0.0)
            acc = acc + dot(p.astype(BF16), v_ref[keys, :])
            carry = carry + jnp.broadcast_to(w[:, 0:1] - kept[:, 0:1], (len_, LANES))
        carry_ref[...] = carry
        acc_ref[...] = acc
        out_ref[to, pl.ds(0, len_), :] = acc.astype(BF16)
        tot_ref[...] = jnp.where(lane == to, carry, tot_ref[...])

    own = x * len_ // half
    part(z, own, None, True)

    def full(i, done):
        j = i - own
        before = i < own
        fresh = jnp.logical_and(jnp.logical_not(before), j % 2 == 0)
        part(
            jnp.where(before, z, z + 1 + j // 2),
            jnp.where(before, 0, 1 - j % 2),
            jnp.where(fresh, 0.0, 1.0),
            False,
        )
        return done

    lax.fori_loop(0, own + 2 * (depth - 1 - z), full, 0)

    def clear(i, done):
        out_ref[i, pl.ds(0, len_), :] = jnp.zeros((len_, hd), BF16)
        return done

    lax.fori_loop(0, z, clear, 0)
    cols = [tot_ref[r * LANES : (r + 1) * LANES, :].T for r in range(n_off)]
    for to in range(depth):
        rest = [col[to : to + 1, :] for col in cols]
        terms = []
        for _ in range(3):
            term = [r.astype(BF16).astype(F32) for r in rest]
            rest = [r - t for r, t in zip(rest, term)]
            terms += term
        terms.append(jnp.zeros((16 - len(terms), LANES), F32))
        out_ref[to, pl.ds(len_, 16), :] = jnp.concatenate(terms, axis=0).astype(BF16)


def join_kernel(depth, len_, in_ref, out_ref, scale_ref):
    n_off = len_ // LANES
    later = [jnp.zeros((1, LANES), F32)] * n_off
    scale_ref[...] = jnp.zeros_like(scale_ref)
    for at in reversed(range(depth)):
        t = in_ref[at, pl.ds(len_, 16), :].astype(F32)
        for r in range(n_off):
            scale_ref[at : at + 1, r * LANES : (r + 1) * LANES] = jnp.exp2(later[r])
            for term in range(3):
                i = term * n_off + r
                later[r] = later[r] + t[i : i + 1, :]
    for r in range(n_off):
        rows = slice(r * LANES, (r + 1) * LANES)
        cols = scale_ref[:, rows].T
        acc = jnp.zeros((LANES, out_ref.shape[1]), F32)
        for at in range(depth):
            acc = acc + in_ref[at, rows, :].astype(F32) * cols[:, at : at + 1]
        out_ref[rows, :] = acc.astype(out_ref.dtype)


def vmem(n):
    return [pl.BlockSpec(memory_space=pltpu.VMEM)] * n


SMEM = pl.BlockSpec(memory_space=pltpu.SMEM)


def dispatch_kernel(cap, at_ref, rows_ref, gain_ref, ids_ref, wts_ref, out_ref, hi_ref, lo_ref):
    tok, slots = rows_ref.shape[0], out_ref.shape[0]
    rows = rows_ref[...].astype(F32)
    rms = lax.rsqrt(jnp.mean(rows * rows, axis=1, keepdims=True) + EPSILON)
    first, second = ids_ref[0:1, :], ids_ref[1:2, :]
    expert = lax.broadcasted_iota(jnp.int32, (LANES, tok), 0)
    chosen = jnp.where((first == expert) | (second == expert), 1.0, 0.0).astype(BF16)
    before = lax.broadcasted_iota(jnp.int32, (tok, tok), 0) < lax.broadcasted_iota(
        jnp.int32, (tok, tok), 1
    )
    rank = dot(chosen, jnp.where(before, 1.0, 0.0).astype(BF16)).astype(BF16)
    spread = (
        lax.broadcasted_iota(jnp.int32, (slots, LANES), 0) // cap
        == lax.broadcasted_iota(jnp.int32, (slots, LANES), 1)
    )
    spread = jnp.where(spread, 1.0, 0.0).astype(BF16)
    slot = lax.broadcasted_iota(jnp.int32, (slots, tok), 0)
    taken = (dot(spread, chosen) > 0.5) & (dot(spread, rank) == (slot % cap).astype(F32))
    pick = jnp.where(taken, 1.0, 0.0).astype(BF16)
    for i in range(out_ref.shape[1] // LANES):
        own = pl.ds(pl.multiple_of((2 * i + at_ref[0]) * LANES, LANES), LANES)
        normed = (rows_ref[:, own].astype(F32) * rms * gain_ref[:, own]).astype(BF16)
        out_ref[:, i * LANES : (i + 1) * LANES] = dot(pick, normed).astype(BF16)
    weight = jnp.where(slot // cap == first, wts_ref[0:1, :], wts_ref[1:2, :])
    weight = jnp.where(taken, weight, 0.0)
    hi = weight.astype(BF16)
    hi_ref[...] = hi
    lo_ref[...] = (weight - hi.astype(F32)).astype(BF16)


def expert_kernel(at_ref, mine_ref, other_ref, gate_ref, up_ref, down_ref, keep_ref, send_ref, all_ref):
    core = at_ref[0]
    chunks = mine_ref.shape[1] // LANES
    for i in range(chunks):
        here = slice(i * LANES, (i + 1) * LANES)
        all_ref[:, pl.ds(pl.multiple_of((2 * i + core) * LANES, LANES), LANES)] = mine_ref[:, here]
        all_ref[:, pl.ds(pl.multiple_of((2 * i + 1 - core) * LANES, LANES), LANES)] = other_ref[:, here]
    tokens = all_ref[...]
    gate = dot(tokens, gate_ref[...], ((1,), (1,)))
    up = dot(tokens, up_ref[...], ((1,), (1,)))
    hidden = (gate / (1.0 + jnp.exp(-gate)) * up).astype(BF16)
    all_ref[...] = dot(hidden, down_ref[...]).astype(BF16)
    for i in range(chunks):
        keep_ref[i] = all_ref[:, pl.ds(pl.multiple_of((2 * i + core) * LANES, LANES), LANES)]
        send_ref[i] = all_ref[:, pl.ds(pl.multiple_of((2 * i + 1 - core) * LANES, LANES), LANES)]


def sum_kernel(in_ref, out_ref):
    total = in_ref[0].astype(F32)
    for i in range(1, in_ref.shape[0]):
        total = total + in_ref[i].astype(F32)
    out_ref[...] = total.astype(out_ref.dtype)


def combine_kernel(hi_ref, lo_ref, back_ref, out_ref):
    back = back_ref[...]
    out_ref[...] = (
        dot(hi_ref[...], back, ((0,), (0,))) + dot(lo_ref[...], back, ((0,), (0,)))
    ).astype(BF16)


def swap(x):
    return lax.ppermute(x, "core", [(0, 1), (1, 0)])


def layer(
    queries, keys, values, key_offset, rows, gain, gate_w, up_w, down_w, expert_ids, route_weights
):
    experts = lax.axis_size(EP)
    tok, width = rows.shape
    half = width // lax.axis_size("core")
    hosts = lax.axis_size("y")
    cap = 2 * expert_ids.shape[1] * tok // experts
    slots = experts * cap
    depth, wide = lax.axis_size("z"), lax.axis_size("x")
    len_, hd = queries.shape
    core = jnp.stack([lax.axis_index("core")]).astype(jnp.int32)
    place = jnp.stack([lax.axis_index("z"), lax.axis_index("x")]).astype(jnp.int32)
    outgoing, hi, lo = pl.pallas_call(
        functools.partial(dispatch_kernel, cap),
        out_shape=(
            jax.ShapeDtypeStruct((slots, half), BF16),
            jax.ShapeDtypeStruct((slots, tok), BF16),
            jax.ShapeDtypeStruct((slots, tok), BF16),
        ),
        in_specs=[SMEM] + vmem(4),
        out_specs=tuple(vmem(3)),
        name="dispatch",
    )(core, rows, gain.reshape(1, -1), expert_ids.T, route_weights.T)
    mine = lax.all_to_all(outgoing.reshape(experts, cap, half), EP, 0, 0, tiled=True)
    mine = mine.reshape(slots, half)

    off = jnp.pad(key_offset.reshape(-1, LANES), ((0, 16 - len_ // LANES), (0, 0)))
    kvo = [jnp.concatenate([keys, values, off], axis=0)]
    for step in range(1, wide):
        kvo.append(lax.ppermute(kvo[0], "x", [(i, (i + step) % wide) for i in range(wide)]))
    q = lax.all_gather(queries, "z")

    hidden = gate_w.shape[2]
    other = swap(mine)
    keep, send = pl.pallas_call(
        expert_kernel,
        out_shape=(jax.ShapeDtypeStruct((hosts, slots, LANES), BF16),) * 2,
        in_specs=[SMEM] + vmem(5),
        out_specs=tuple(vmem(2)),
        scratch_shapes=[pltpu.VMEM((slots, width), BF16)],
        compiler_params=pltpu.CompilerParams(vmem_limit_bytes=32 << 20),
        cost_estimate=pl.CostEstimate(
            flops=6 * slots * width * hidden,
            transcendentals=slots * hidden,
            bytes_accessed=2 * (2 * slots * width + 3 * width * hidden),
        ),
        name="experts",
    )(core, mine, other, gate_w[0].T, up_w[0].T, down_w[0])
    other = swap(send)
    share = (keep.astype(F32) + other.astype(F32)).astype(BF16)
    share = lax.all_to_all(share, "y", 0, 0, tiled=True)

    sums = pl.pallas_call(
        functools.partial(block_kernel, depth, wide, len_, hd),
        out_shape=jax.ShapeDtypeStruct((depth, len_ + 16, hd), BF16),
        in_specs=[SMEM] + vmem(1 + wide),
        out_specs=vmem(1)[0],
        scratch_shapes=[
            pltpu.VMEM((depth, len_, 2 * hd), BF16),
            pltpu.VMEM((wide * len_, 2 * hd), BF16),
            pltpu.VMEM((wide * len_, hd), BF16),
            pltpu.VMEM((8, wide * len_), F32),
            pltpu.VMEM((TILE, TILE), BF16),
            pltpu.VMEM((len_, LANES), F32),
            pltpu.VMEM((len_, hd), F32),
            pltpu.VMEM((len_, LANES), F32),
        ],
        compiler_params=pltpu.CompilerParams(vmem_limit_bytes=32 << 20),
        cost_estimate=pl.CostEstimate(
            flops=depth * wide * len_ * len_ * (4 * hd + 2 * len_),
            transcendentals=3 * depth * wide * len_ * len_,
            bytes_accessed=2 * (2 * depth * len_ * hd + wide * kvo[0].size),
        ),
        name="stick_blocks",
    )(place, q, *kvo)
    arrived = lax.all_to_all(sums, "z", 0, 0, tiled=True)
    attended = pl.pallas_call(
        functools.partial(join_kernel, depth, len_),
        out_shape=jax.ShapeDtypeStruct((len_, hd), BF16),
        in_specs=vmem(1),
        out_specs=vmem(1)[0],
        scratch_shapes=[pltpu.VMEM((LANES, len_), F32)],
        cost_estimate=pl.CostEstimate(
            flops=2 * depth * len_ * hd, transcendentals=depth * len_, bytes_accessed=2 * depth * len_ * hd
        ),
        name="stick_join",
    )(arrived)

    share = pl.pallas_call(
        sum_kernel,
        out_shape=jax.ShapeDtypeStruct((slots, LANES), BF16),
        in_specs=vmem(1),
        out_specs=vmem(1)[0],
        name="parts_sum",
    )(share)
    back = lax.all_to_all(share.reshape(experts, cap, LANES), EP, 0, 0, tiled=True)
    mixed = pl.pallas_call(
        combine_kernel,
        out_shape=jax.ShapeDtypeStruct((tok, LANES), BF16),
        in_specs=vmem(3),
        out_specs=vmem(1)[0],
        name="combine",
    )(hi, lo, back.reshape(slots, LANES))
    mixed = lax.all_gather(mixed, TP, axis=1, tiled=True)
    return (attended, mixed)


def solution(mesh):
    fine = Mesh(mesh.devices.reshape(Z, X, Y, CORE), ("z", "x", "y", "core"))
    return jax.shard_map(
        layer,
        mesh=fine,
        in_specs=(
            P(EP, TP),
            P(EP, TP),
            P(EP, TP),
            P(EP, TP),
            P(EP, None),
            P(),
            P(EP, None, TP),
            P(EP, None, TP),
            P(EP, TP, None),
            P(EP, None),
            P(EP, None),
        ),
        out_specs=(P(EP, TP), P(EP, None)),
        check_vma=False,
    )
```

```python
import functools

import jax
import jax.numpy as jnp
from jax import lax
from jax.experimental import pallas as pl
from jax.experimental.pallas import tpu as pltpu
from jax.sharding import Mesh
from jax.sharding import PartitionSpec as P


EPSILON = 1e-06
LOG2E = 1.4426950408889634
F32 = jnp.float32
BF16 = jnp.bfloat16
ZH, ZL, X, Y, CORE = 4, 2, 4, 8, 2
Z = ("zh", "zl")
EP = (*Z, "x")
TP = ("y", "core")
LANES = 128
TILE = 256


def dot(a, b, dims=((1,), (0,))):
    return lax.dot_general(a, b, (dims, ((), ())), preferred_element_type=F32)


def block_kernel(depth, width, len_, hd, at_ref, q_ref, *refs):
    near, (out_ref, qq_ref, kk_ref, v_ref, off_ref, tri_ref, tot_ref, acc_ref, carry_ref) = (
        refs[:width],
        refs[width:],
    )
    z, x = at_ref[0], at_ref[1]
    n_off = len_ // LANES
    half = width * len_ // 2
    for step in range(width):
        rows = pl.ds(pl.multiple_of((x + width - step) % width * len_, len_), len_)
        for twice in range(2):
            kk_ref[rows, twice * hd : (twice + 1) * hd] = near[step][:len_, :]
        v_ref[rows, :] = near[step][len_ : 2 * len_, :]
        o = near[step][2 * len_ :, :].astype(F32) * LOG2E
        for i in range(n_off):
            at = pl.ds(pl.multiple_of(((x + width - step) % width * n_off + i) * LANES, LANES), LANES)
            off_ref[0:1, at] = o[i : i + 1, :]

    def scale(i, done):
        q = q_ref[i // 2 * 2 + (i + z) % 2].astype(F32) * (hd**-0.5 * LOG2E)
        hi = q.astype(BF16)
        qq_ref[i, :, :hd] = hi
        qq_ref[i, :, hd:] = (q - hi.astype(F32)).astype(BF16)
        return done

    lax.fori_loop(z, depth, scale, 0)
    tri_ref[...] = jnp.where(
        lax.broadcasted_iota(jnp.int32, (TILE, TILE), 0) > lax.broadcasted_iota(jnp.int32, (TILE, TILE), 1),
        -1.0,
        0.0,
    ).astype(BF16)
    tot_ref[...] = jnp.zeros_like(tot_ref)
    lane = lax.broadcasted_iota(jnp.int32, (len_, LANES), 1)

    def part(to, which, old, masked):
        start = pl.multiple_of(which * half, half)
        q = qq_ref[to]
        carry = 0.0 if masked else carry_ref[...] * old
        acc = 0.0 if masked else acc_ref[...] * old
        for tile in reversed(range(half // TILE)):
            keys = pl.ds(pl.multiple_of(start + tile * TILE, TILE), TILE)
            u = dot(q, kk_ref[keys, :], ((1,), (1,))) + off_ref[0:1, keys]
            sp = kept = jnp.maximum(u, 0.0) + jnp.log2(1.0 + jnp.exp2(-jnp.abs(u)))
            if masked:
                ahead = lax.broadcasted_iota(jnp.int32, (len_, TILE), 0) - lax.broadcasted_iota(
                    jnp.int32, (len_, TILE), 1
                )
                strict = ahead > start + tile * TILE - x * len_
                kept = jnp.where(strict, sp, 0.0)
            w = dot(kept.astype(BF16), tri_ref[...])
            if isinstance(carry, float):
                p = jnp.exp2(u - sp + w)
            else:
                p = jnp.exp2(u - sp + w + jnp.concatenate([carry] * (TILE // LANES), axis=1))
            if masked:
                p = jnp.where(strict, p, 0.0)
            acc = acc + dot(p.astype(BF16), v_ref[keys, :])
            carry = carry + jnp.broadcast_to(w[:, 0:1] - kept[:, 0:1], (len_, LANES))
        carry_ref[...] = carry
        acc_ref[...] = acc
        out_ref[to, pl.ds(0, len_), :] = acc.astype(BF16)
        tot_ref[...] = jnp.where(lane == to, carry, tot_ref[...])

    own = x * len_ // half
    part(z, own, None, True)

    def full(i, done):
        j = i - own
        before = i < own
        fresh = jnp.logical_and(jnp.logical_not(before), j % 2 == 0)
        part(
            jnp.where(before, z, z + 1 + j // 2),
            jnp.where(before, 0, 1 - j % 2),
            jnp.where(fresh, 0.0, 1.0),
            False,
        )
        return done

    lax.fori_loop(0, own + 2 * (depth - 1 - z), full, 0)

    def clear(i, done):
        out_ref[i, pl.ds(0, len_), :] = jnp.zeros((len_, hd), BF16)
        return done

    lax.fori_loop(0, z, clear, 0)
    cols = [tot_ref[r * LANES : (r + 1) * LANES, :].T for r in range(n_off)]
    for to in range(depth):
        rest = [col[to : to + 1, :] for col in cols]
        terms = []
        for _ in range(3):
            term = [r.astype(BF16).astype(F32) for r in rest]
            rest = [r - t for r, t in zip(rest, term)]
            terms += term
        terms.append(jnp.zeros((16 - len(terms), LANES), F32))
        out_ref[to, pl.ds(len_, 16), :] = jnp.concatenate(terms, axis=0).astype(BF16)


def join_kernel(depth, len_, in_ref, out_ref, scale_ref):
    n_off = len_ // LANES
    later = [jnp.zeros((1, LANES), F32)] * n_off
    scale_ref[...] = jnp.zeros_like(scale_ref)
    for at in reversed(range(depth)):
        t = in_ref[at, pl.ds(len_, 16), :].astype(F32)
        for r in range(n_off):
            scale_ref[at : at + 1, r * LANES : (r + 1) * LANES] = jnp.exp2(later[r])
            for term in range(3):
                i = term * n_off + r
                later[r] = later[r] + t[i : i + 1, :]
    for r in range(n_off):
        rows = slice(r * LANES, (r + 1) * LANES)
        cols = scale_ref[:, rows].T
        acc = jnp.zeros((LANES, out_ref.shape[1]), F32)
        for at in range(depth):
            acc = acc + in_ref[at, rows, :].astype(F32) * cols[:, at : at + 1]
        out_ref[rows, :] = acc.astype(out_ref.dtype)


def vmem(n):
    return [pl.BlockSpec(memory_space=pltpu.VMEM)] * n


SMEM = pl.BlockSpec(memory_space=pltpu.SMEM)


def dispatch_kernel(cap, at_ref, rows_ref, gain_ref, ids_ref, wts_ref, out_ref, hi_ref, lo_ref):
    tok, slots = rows_ref.shape[0], out_ref.shape[0]
    rows = rows_ref[...].astype(F32)
    rms = lax.rsqrt(jnp.mean(rows * rows, axis=1, keepdims=True) + EPSILON)
    first, second = ids_ref[0:1, :], ids_ref[1:2, :]
    expert = lax.broadcasted_iota(jnp.int32, (LANES, tok), 0)
    chosen = jnp.where((first == expert) | (second == expert), 1.0, 0.0).astype(BF16)
    before = lax.broadcasted_iota(jnp.int32, (tok, tok), 0) < lax.broadcasted_iota(
        jnp.int32, (tok, tok), 1
    )
    rank = dot(chosen, jnp.where(before, 1.0, 0.0).astype(BF16)).astype(BF16)
    spread = (
        lax.broadcasted_iota(jnp.int32, (slots, LANES), 0) // cap
        == lax.broadcasted_iota(jnp.int32, (slots, LANES), 1)
    )
    spread = jnp.where(spread, 1.0, 0.0).astype(BF16)
    slot = lax.broadcasted_iota(jnp.int32, (slots, tok), 0)
    taken = (dot(spread, chosen) > 0.5) & (dot(spread, rank) == (slot % cap).astype(F32))
    pick = jnp.where(taken, 1.0, 0.0).astype(BF16)
    for i in range(out_ref.shape[1] // LANES):
        own = pl.ds(pl.multiple_of((2 * i + at_ref[0]) * LANES, LANES), LANES)
        normed = (rows_ref[:, own].astype(F32) * rms * gain_ref[:, own]).astype(BF16)
        out_ref[:, i * LANES : (i + 1) * LANES] = dot(pick, normed).astype(BF16)
    weight = jnp.where(slot // cap == first, wts_ref[0:1, :], wts_ref[1:2, :])
    weight = jnp.where(taken, weight, 0.0)
    hi = weight.astype(BF16)
    hi_ref[...] = hi
    lo_ref[...] = (weight - hi.astype(F32)).astype(BF16)


def expert_kernel(at_ref, mine_ref, other_ref, gate_ref, up_ref, down_ref, keep_ref, send_ref, all_ref):
    core = at_ref[0]
    chunks = mine_ref.shape[1] // LANES
    for i in range(chunks):
        here = slice(i * LANES, (i + 1) * LANES)
        all_ref[:, pl.ds(pl.multiple_of((2 * i + core) * LANES, LANES), LANES)] = mine_ref[:, here]
        all_ref[:, pl.ds(pl.multiple_of((2 * i + 1 - core) * LANES, LANES), LANES)] = other_ref[:, here]
    tokens = all_ref[...]
    gate = dot(tokens, gate_ref[...], ((1,), (1,)))
    up = dot(tokens, up_ref[...], ((1,), (1,)))
    hidden = (gate / (1.0 + jnp.exp(-gate)) * up).astype(BF16)
    all_ref[...] = dot(hidden, down_ref[...]).astype(BF16)
    for i in range(chunks):
        for to_ref, half in ((keep_ref, core), (send_ref, 1 - core)):
            cols = pl.ds(pl.multiple_of((2 * i + half) * LANES, LANES), LANES)
            to_ref[:, i] = all_ref[:, cols].reshape(to_ref.shape[0], to_ref.shape[2], LANES)


def combine_kernel(hi_ref, lo_ref, back_ref, out_ref):
    total = back_ref[:, 0].astype(F32)
    for i in range(1, back_ref.shape[1]):
        total = total + back_ref[:, i].astype(F32)
    total = total.astype(BF16).reshape(-1, LANES)
    out_ref[...] = (
        dot(hi_ref[...], total, ((0,), (0,))) + dot(lo_ref[...], total, ((0,), (0,)))
    ).astype(BF16)


def swap(x):
    return lax.ppermute(x, "core", [(0, 1), (1, 0)])


def layer(
    queries, keys, values, key_offset, rows, gain, gate_w, up_w, down_w, expert_ids, route_weights
):
    experts = lax.axis_size(EP)
    tok, width = rows.shape
    half = width // lax.axis_size("core")
    hosts = lax.axis_size("y")
    cap = 2 * expert_ids.shape[1] * tok // experts
    slots = experts * cap
    depth, wide = lax.axis_size(Z), lax.axis_size("x")
    len_, hd = queries.shape
    core = jnp.stack([lax.axis_index("core")]).astype(jnp.int32)
    place = jnp.stack([lax.axis_index(Z), lax.axis_index("x")]).astype(jnp.int32)
    outgoing, hi, lo = pl.pallas_call(
        functools.partial(dispatch_kernel, cap),
        out_shape=(
            jax.ShapeDtypeStruct((slots, half), BF16),
            jax.ShapeDtypeStruct((slots, tok), BF16),
            jax.ShapeDtypeStruct((slots, tok), BF16),
        ),
        in_specs=[SMEM] + vmem(4),
        out_specs=tuple(vmem(3)),
        name="dispatch",
    )(core, rows, gain.reshape(1, -1), expert_ids.T, route_weights.T)
    mine = lax.all_to_all(outgoing.reshape(experts, cap, half), EP, 0, 0, tiled=True)
    mine = mine.reshape(slots, half)

    off = jnp.pad(key_offset.reshape(-1, LANES), ((0, 16 - len_ // LANES), (0, 0)))
    kvo = [jnp.concatenate([keys, values, off], axis=0)]
    for step in range(1, wide):
        kvo.append(lax.ppermute(kvo[0], "x", [(i, (i + step) % wide) for i in range(wide)]))
    q = lax.ppermute(queries, "zl", [(0, 1), (1, 0)])
    q = jnp.concatenate([queries, q], axis=0)
    q = lax.all_gather(q, "zh").reshape(depth, len_, hd)

    hidden = gate_w.shape[2]
    other = swap(mine)
    keep, send = pl.pallas_call(
        expert_kernel,
        out_shape=(jax.ShapeDtypeStruct((experts, hosts, cap, LANES), BF16),) * 2,
        in_specs=[SMEM] + vmem(5),
        out_specs=tuple(vmem(2)),
        scratch_shapes=[pltpu.VMEM((slots, width), BF16)],
        compiler_params=pltpu.CompilerParams(vmem_limit_bytes=32 << 20),
        cost_estimate=pl.CostEstimate(
            flops=6 * slots * width * hidden,
            transcendentals=slots * hidden,
            bytes_accessed=2 * (2 * slots * width + 3 * width * hidden),
        ),
        name="experts",
    )(core, mine, other, gate_w[0].T, up_w[0].T, down_w[0])
    other = swap(send)
    share = (keep.astype(F32) + other.astype(F32)).astype(BF16)
    back = lax.all_to_all(share.reshape(-1, cap, LANES), (*EP, "y"), 0, 0, tiled=True)

    sums = pl.pallas_call(
        functools.partial(block_kernel, depth, wide, len_, hd),
        out_shape=jax.ShapeDtypeStruct((depth, len_ + 16, hd), BF16),
        in_specs=[SMEM] + vmem(1 + wide),
        out_specs=vmem(1)[0],
        scratch_shapes=[
            pltpu.VMEM((depth, len_, 2 * hd), BF16),
            pltpu.VMEM((wide * len_, 2 * hd), BF16),
            pltpu.VMEM((wide * len_, hd), BF16),
            pltpu.VMEM((8, wide * len_), F32),
            pltpu.VMEM((TILE, TILE), BF16),
            pltpu.VMEM((len_, LANES), F32),
            pltpu.VMEM((len_, hd), F32),
            pltpu.VMEM((len_, LANES), F32),
        ],
        compiler_params=pltpu.CompilerParams(vmem_limit_bytes=32 << 20),
        cost_estimate=pl.CostEstimate(
            flops=depth * wide * len_ * len_ * (4 * hd + 2 * len_),
            transcendentals=3 * depth * wide * len_ * len_,
            bytes_accessed=2 * (2 * depth * len_ * hd + wide * kvo[0].size),
        ),
        name="stick_blocks",
    )(place, q, *kvo)
    arrived = lax.all_to_all(sums, Z, 0, 0, tiled=True)
    attended = pl.pallas_call(
        functools.partial(join_kernel, depth, len_),
        out_shape=jax.ShapeDtypeStruct((len_, hd), BF16),
        in_specs=vmem(1),
        out_specs=vmem(1)[0],
        scratch_shapes=[pltpu.VMEM((LANES, len_), F32)],
        cost_estimate=pl.CostEstimate(
            flops=2 * depth * len_ * hd, transcendentals=depth * len_, bytes_accessed=2 * depth * len_ * hd
        ),
        name="stick_join",
    )(arrived)

    mixed = pl.pallas_call(
        combine_kernel,
        out_shape=jax.ShapeDtypeStruct((tok, LANES), BF16),
        in_specs=vmem(3),
        out_specs=vmem(1)[0],
        name="combine",
    )(hi, lo, back.reshape(experts, hosts, cap, LANES))
    mixed = lax.all_gather(mixed, TP, axis=1, tiled=True)
    return (attended, mixed)


def solution(mesh):
    fine = Mesh(mesh.devices.reshape(ZH, ZL, X, Y, CORE), (*Z, "x", *TP))
    return jax.shard_map(
        layer,
        mesh=fine,
        in_specs=(
            P(EP, TP),
            P(EP, TP),
            P(EP, TP),
            P(EP, TP),
            P(EP, None),
            P(),
            P(EP, None, TP),
            P(EP, None, TP),
            P(EP, TP, None),
            P(EP, None),
            P(EP, None),
        ),
        out_specs=(P(EP, TP), P(EP, None)),
        check_vma=False,
    )
```

```python
import functools

import jax
import jax.numpy as jnp
from jax import lax
from jax.experimental import pallas as pl
from jax.experimental.pallas import tpu as pltpu
from jax.sharding import Mesh
from jax.sharding import PartitionSpec as P


EPSILON = 1e-06
LOG2E = 1.4426950408889634
F32 = jnp.float32
BF16 = jnp.bfloat16
ZH, ZL, X, Y, CORE = 4, 2, 4, 8, 2
Z = ("zh", "zl")
EP = (*Z, "x")
TP = ("y", "core")
LANES = 128
TILE = 256


def dot(a, b, dims=((1,), (0,))):
    return lax.dot_general(a, b, (dims, ((), ())), preferred_element_type=F32)


def block_kernel(depth, width, len_, hd, at_ref, q_ref, *refs):
    near, (out_ref, qq_ref, kk_ref, v_ref, off_ref, tri_ref, tot_ref, acc_ref, carry_ref) = (
        refs[:width],
        refs[width:],
    )
    z, x = at_ref[0], at_ref[1]
    n_off = len_ // LANES
    half = width * len_ // 2
    for step in range(width):
        rows = pl.ds(pl.multiple_of((x + width - step) % width * len_, len_), len_)
        for twice in range(2):
            kk_ref[rows, twice * hd : (twice + 1) * hd] = near[step][:len_, :]
        v_ref[rows, :] = near[step][len_ : 2 * len_, :]
        o = near[step][2 * len_ :, :].astype(F32) * LOG2E
        for i in range(n_off):
            at = pl.ds(pl.multiple_of(((x + width - step) % width * n_off + i) * LANES, LANES), LANES)
            off_ref[0:1, at] = o[i : i + 1, :]

    def scale(i, done):
        q = q_ref[i // 2 * 2 + (i + z) % 2].astype(F32) * (hd**-0.5 * LOG2E)
        hi = q.astype(BF16)
        qq_ref[i, :, :hd] = hi
        qq_ref[i, :, hd:] = (q - hi.astype(F32)).astype(BF16)
        return done

    lax.fori_loop(z, depth, scale, 0)
    tri_ref[...] = jnp.where(
        lax.broadcasted_iota(jnp.int32, (TILE, TILE), 0) > lax.broadcasted_iota(jnp.int32, (TILE, TILE), 1),
        -1.0,
        0.0,
    ).astype(BF16)
    tot_ref[...] = jnp.zeros_like(tot_ref)
    lane = lax.broadcasted_iota(jnp.int32, (len_, LANES), 1)

    def part(to, start, tiles, carry, acc, masked):
        q = qq_ref[to]
        for tile in reversed(range(tiles)):
            keys = pl.ds(pl.multiple_of(start + tile * TILE, TILE), TILE)
            u = dot(q, kk_ref[keys, :], ((1,), (1,))) + off_ref[0:1, keys]
            sp = kept = jnp.maximum(u, jnp.log2(1.0 + jnp.exp2(jnp.minimum(u, 126.0))))
            if masked:
                ahead = lax.broadcasted_iota(jnp.int32, (len_, TILE), 0) - lax.broadcasted_iota(
                    jnp.int32, (len_, TILE), 1
                )
                strict = ahead > start + tile * TILE - x * len_
                kept = jnp.where(strict, sp, 0.0)
            w = dot(kept.astype(BF16), tri_ref[...])
            if carry is None:
                p = jnp.exp2(u - sp + w)
            else:
                p = jnp.exp2(u - sp + w + jnp.concatenate([carry] * (TILE // LANES), axis=1))
            if masked:
                p = jnp.where(strict, p, 0.0)
            summed = dot(p.astype(BF16), v_ref[keys, :])
            total = jnp.broadcast_to(w[:, 0:1] - kept[:, 0:1], (len_, LANES))
            acc = summed if acc is None else acc + summed
            carry = total if carry is None else carry + total
        out_ref[to, pl.ds(0, len_), :] = acc.astype(BF16)
        tot_ref[...] = jnp.where(lane == to, carry, tot_ref[...])
        return carry, acc

    own = x * len_ // half
    carry_ref[...], acc_ref[...] = part(z, own * half, half // TILE, None, None, True)

    @pl.when(own == 1)
    def _():
        part(z, 0, half // TILE, carry_ref[...], acc_ref[...], False)

    def full(i, done):
        part(i, 0, 2 * half // TILE, None, None, False)
        return done

    lax.fori_loop(z + 1, depth, full, 0)

    def clear(i, done):
        out_ref[i, pl.ds(0, len_), :] = jnp.zeros((len_, hd), BF16)
        return done

    lax.fori_loop(0, z, clear, 0)
    cols = [tot_ref[r * LANES : (r + 1) * LANES, :].T for r in range(n_off)]
    for to in range(depth):
        rest = [col[to : to + 1, :] for col in cols]
        terms = []
        for _ in range(3):
            term = [r.astype(BF16).astype(F32) for r in rest]
            rest = [r - t for r, t in zip(rest, term)]
            terms += term
        terms.append(jnp.zeros((16 - len(terms), LANES), F32))
        out_ref[to, pl.ds(len_, 16), :] = jnp.concatenate(terms, axis=0).astype(BF16)


def join_kernel(depth, len_, in_ref, out_ref, scale_ref):
    n_off = len_ // LANES
    later = [jnp.zeros((1, LANES), F32)] * n_off
    scale_ref[...] = jnp.zeros_like(scale_ref)
    for at in reversed(range(depth)):
        t = in_ref[at, pl.ds(len_, 16), :].astype(F32)
        for r in range(n_off):
            scale_ref[at : at + 1, r * LANES : (r + 1) * LANES] = jnp.exp2(later[r])
            for term in range(3):
                i = term * n_off + r
                later[r] = later[r] + t[i : i + 1, :]
    for r in range(n_off):
        rows = slice(r * LANES, (r + 1) * LANES)
        cols = scale_ref[:, rows].T
        acc = jnp.zeros((LANES, out_ref.shape[1]), F32)
        for at in range(depth):
            acc = acc + in_ref[at, rows, :].astype(F32) * cols[:, at : at + 1]
        out_ref[rows, :] = acc.astype(out_ref.dtype)


def vmem(n):
    return [pl.BlockSpec(memory_space=pltpu.VMEM)] * n


SMEM = pl.BlockSpec(memory_space=pltpu.SMEM)


def dispatch_kernel(cap, at_ref, rows_ref, gain_ref, ids_ref, wts_ref, out_ref, hi_ref, lo_ref):
    tok, slots = rows_ref.shape[0], out_ref.shape[0]
    rows = rows_ref[...].astype(F32)
    rms = lax.rsqrt(jnp.mean(rows * rows, axis=1, keepdims=True) + EPSILON)
    first, second = ids_ref[0:1, :], ids_ref[1:2, :]
    expert = lax.broadcasted_iota(jnp.int32, (LANES, tok), 0)
    chosen = jnp.where((first == expert) | (second == expert), 1.0, 0.0).astype(BF16)
    before = lax.broadcasted_iota(jnp.int32, (tok, tok), 0) < lax.broadcasted_iota(
        jnp.int32, (tok, tok), 1
    )
    rank = dot(chosen, jnp.where(before, 1.0, 0.0).astype(BF16)).astype(BF16)
    spread = (
        lax.broadcasted_iota(jnp.int32, (slots, LANES), 0) // cap
        == lax.broadcasted_iota(jnp.int32, (slots, LANES), 1)
    )
    spread = jnp.where(spread, 1.0, 0.0).astype(BF16)
    slot = lax.broadcasted_iota(jnp.int32, (slots, tok), 0)
    taken = (dot(spread, chosen) > 0.5) & (dot(spread, rank) == (slot % cap).astype(F32))
    pick = jnp.where(taken, 1.0, 0.0).astype(BF16)
    for i in range(out_ref.shape[1] // LANES):
        own = pl.ds(pl.multiple_of((2 * i + at_ref[0]) * LANES, LANES), LANES)
        normed = (rows_ref[:, own].astype(F32) * rms * gain_ref[:, own]).astype(BF16)
        out_ref[:, i * LANES : (i + 1) * LANES] = dot(pick, normed).astype(BF16)
    weight = jnp.where(slot // cap == first, wts_ref[0:1, :], wts_ref[1:2, :])
    weight = jnp.where(taken, weight, 0.0)
    hi = weight.astype(BF16)
    hi_ref[...] = hi
    lo_ref[...] = (weight - hi.astype(F32)).astype(BF16)


def expert_kernel(at_ref, mine_ref, other_ref, gate_ref, up_ref, down_ref, keep_ref, send_ref, all_ref):
    core = at_ref[0]
    chunks = mine_ref.shape[1] // LANES
    for i in range(chunks):
        here = slice(i * LANES, (i + 1) * LANES)
        all_ref[:, pl.ds(pl.multiple_of((2 * i + core) * LANES, LANES), LANES)] = mine_ref[:, here]
        all_ref[:, pl.ds(pl.multiple_of((2 * i + 1 - core) * LANES, LANES), LANES)] = other_ref[:, here]
    tokens = all_ref[...]
    gate = dot(tokens, gate_ref[...], ((1,), (1,)))
    up = dot(tokens, up_ref[...], ((1,), (1,)))
    hidden = (gate / (1.0 + jnp.exp(-gate)) * up).astype(BF16)
    all_ref[...] = dot(hidden, down_ref[...]).astype(BF16)
    for i in range(chunks):
        keep_ref[i] = all_ref[:, pl.ds(pl.multiple_of((2 * i + core) * LANES, LANES), LANES)]
        send_ref[i] = all_ref[:, pl.ds(pl.multiple_of((2 * i + 1 - core) * LANES, LANES), LANES)]


def sum_kernel(in_ref, out_ref):
    total = in_ref[0].astype(F32)
    for i in range(1, in_ref.shape[0]):
        total = total + in_ref[i].astype(F32)
    out_ref[...] = total.astype(out_ref.dtype)


def combine_kernel(hi_ref, lo_ref, back_ref, out_ref):
    back = back_ref[...]
    out_ref[...] = (
        dot(hi_ref[...], back, ((0,), (0,))) + dot(lo_ref[...], back, ((0,), (0,)))
    ).astype(BF16)


def swap(x):
    return lax.ppermute(x, "core", [(0, 1), (1, 0)])


def layer(
    queries, keys, values, key_offset, rows, gain, gate_w, up_w, down_w, expert_ids, route_weights
):
    experts = lax.axis_size(EP)
    tok, width = rows.shape
    half = width // lax.axis_size("core")
    hosts = lax.axis_size("y")
    cap = 2 * expert_ids.shape[1] * tok // experts
    slots = experts * cap
    depth, wide = lax.axis_size(Z), lax.axis_size("x")
    len_, hd = queries.shape
    core = jnp.stack([lax.axis_index("core")]).astype(jnp.int32)
    place = jnp.stack([lax.axis_index(Z), lax.axis_index("x")]).astype(jnp.int32)
    outgoing, hi, lo = pl.pallas_call(
        functools.partial(dispatch_kernel, cap),
        out_shape=(
            jax.ShapeDtypeStruct((slots, half), BF16),
            jax.ShapeDtypeStruct((slots, tok), BF16),
            jax.ShapeDtypeStruct((slots, tok), BF16),
        ),
        in_specs=[SMEM] + vmem(4),
        out_specs=tuple(vmem(3)),
        name="dispatch",
    )(core, rows, gain.reshape(1, -1), expert_ids.T, route_weights.T)
    mine = lax.all_to_all(outgoing.reshape(experts, cap, half), EP, 0, 0, tiled=True)
    mine = mine.reshape(slots, half)

    off = jnp.pad(key_offset.reshape(-1, LANES), ((0, 16 - len_ // LANES), (0, 0)))
    kvo = [jnp.concatenate([keys, values, off], axis=0)]
    for step in range(1, wide):
        kvo.append(lax.ppermute(kvo[0], "x", [(i, (i + step) % wide) for i in range(wide)]))
    q = lax.ppermute(queries, "zl", [(0, 1), (1, 0)])
    q = jnp.concatenate([queries, q], axis=0)
    q = lax.all_gather(q, "zh").reshape(depth, len_, hd)

    hidden = gate_w.shape[2]
    other = swap(mine)
    keep, send = pl.pallas_call(
        expert_kernel,
        out_shape=(jax.ShapeDtypeStruct((hosts, slots, LANES), BF16),) * 2,
        in_specs=[SMEM] + vmem(5),
        out_specs=tuple(vmem(2)),
        scratch_shapes=[pltpu.VMEM((slots, width), BF16)],
        compiler_params=pltpu.CompilerParams(vmem_limit_bytes=32 << 20),
        cost_estimate=pl.CostEstimate(
            flops=6 * slots * width * hidden,
            transcendentals=slots * hidden,
            bytes_accessed=2 * (2 * slots * width + 3 * width * hidden),
        ),
        name="experts",
    )(core, mine, other, gate_w[0].T, up_w[0].T, down_w[0])
    other = swap(send)
    share = (keep.astype(F32) + other.astype(F32)).astype(BF16)
    share = lax.all_to_all(share, "y", 0, 0, tiled=True)

    sums = pl.pallas_call(
        functools.partial(block_kernel, depth, wide, len_, hd),
        out_shape=jax.ShapeDtypeStruct((depth, len_ + 16, hd), BF16),
        in_specs=[SMEM] + vmem(1 + wide),
        out_specs=vmem(1)[0],
        scratch_shapes=[
            pltpu.VMEM((depth, len_, 2 * hd), BF16),
            pltpu.VMEM((wide * len_, 2 * hd), BF16),
            pltpu.VMEM((wide * len_, hd), BF16),
            pltpu.VMEM((8, wide * len_), F32),
            pltpu.VMEM((TILE, TILE), BF16),
            pltpu.VMEM((len_, LANES), F32),
            pltpu.VMEM((len_, hd), F32),
            pltpu.VMEM((len_, LANES), F32),
        ],
        compiler_params=pltpu.CompilerParams(vmem_limit_bytes=32 << 20),
        cost_estimate=pl.CostEstimate(
            flops=depth * wide * len_ * len_ * (4 * hd + 2 * len_),
            transcendentals=3 * depth * wide * len_ * len_,
            bytes_accessed=2 * (2 * depth * len_ * hd + wide * kvo[0].size),
        ),
        name="stick_blocks",
    )(place, q, *kvo)
    arrived = lax.all_to_all(sums, Z, 0, 0, tiled=True)
    attended = pl.pallas_call(
        functools.partial(join_kernel, depth, len_),
        out_shape=jax.ShapeDtypeStruct((len_, hd), BF16),
        in_specs=vmem(1),
        out_specs=vmem(1)[0],
        scratch_shapes=[pltpu.VMEM((LANES, len_), F32)],
        cost_estimate=pl.CostEstimate(
            flops=2 * depth * len_ * hd, transcendentals=depth * len_, bytes_accessed=2 * depth * len_ * hd
        ),
        name="stick_join",
    )(arrived)

    share = pl.pallas_call(
        sum_kernel,
        out_shape=jax.ShapeDtypeStruct((slots, LANES), BF16),
        in_specs=vmem(1),
        out_specs=vmem(1)[0],
        name="parts_sum",
    )(share)
    back = lax.all_to_all(share.reshape(experts, cap, LANES), EP, 0, 0, tiled=True)
    mixed = pl.pallas_call(
        combine_kernel,
        out_shape=jax.ShapeDtypeStruct((tok, LANES), BF16),
        in_specs=vmem(3),
        out_specs=vmem(1)[0],
        name="combine",
    )(hi, lo, back.reshape(slots, LANES))
    mixed = lax.all_gather(mixed, TP, axis=1, tiled=True)
    return (attended, mixed)


def solution(mesh):
    fine = Mesh(mesh.devices.reshape(ZH, ZL, X, Y, CORE), (*Z, "x", *TP))
    return jax.shard_map(
        layer,
        mesh=fine,
        in_specs=(
            P(EP, TP),
            P(EP, TP),
            P(EP, TP),
            P(EP, TP),
            P(EP, None),
            P(),
            P(EP, None, TP),
            P(EP, None, TP),
            P(EP, TP, None),
            P(EP, None),
            P(EP, None),
        ),
        out_specs=(P(EP, TP), P(EP, None)),
        check_vma=False,
    )
```

```python
import functools

import jax
import jax.numpy as jnp
from jax import lax
from jax.experimental import pallas as pl
from jax.experimental.pallas import tpu as pltpu
from jax.sharding import Mesh
from jax.sharding import PartitionSpec as P


EPSILON = 1e-06
LOG2E = 1.4426950408889634
F32 = jnp.float32
BF16 = jnp.bfloat16
ZH, ZL, X, Y, CORE = 4, 2, 4, 8, 2
Z = ("zh", "zl")
EP = (*Z, "x")
TP = ("y", "core")
LANES = 128
TILE = 256


def dot(a, b, dims=((1,), (0,))):
    return lax.dot_general(a, b, (dims, ((), ())), preferred_element_type=F32)


def block_kernel(depth, width, len_, hd, cut, rest, at_ref, q_ref, *refs):
    if rest:
        prev_ref, *refs = refs
        refs[width][...] = prev_ref[...]
    near, (out_ref, qq_ref, kk_ref, v_ref, off_ref, tri_ref, tot_ref, acc_ref, carry_ref) = (
        refs[:width],
        refs[width:],
    )
    z, x = at_ref[0], at_ref[1]
    low = jnp.maximum(z + 1, cut) if rest else z + 1
    high = depth if rest else cut
    n_off = len_ // LANES
    half = width * len_ // 2
    for step in range(width):
        rows = pl.ds(pl.multiple_of((x + width - step) % width * len_, len_), len_)
        for twice in range(2):
            kk_ref[rows, twice * hd : (twice + 1) * hd] = near[step][:len_, :]
        v_ref[rows, :] = near[step][len_ : 2 * len_, :]
        o = near[step][2 * len_ :, :].astype(F32) * LOG2E
        for i in range(n_off):
            at = pl.ds(pl.multiple_of(((x + width - step) % width * n_off + i) * LANES, LANES), LANES)
            off_ref[0:1, at] = o[i : i + 1, :]

    def scale(i, done):
        q = q_ref[i // 2 * 2 + (i + z) % 2].astype(F32) * (hd**-0.5 * LOG2E)
        hi = q.astype(BF16)
        qq_ref[i, :, :hd] = hi
        qq_ref[i, :, hd:] = (q - hi.astype(F32)).astype(BF16)
        return done

    lax.fori_loop(low if rest else z, high if rest else jnp.maximum(z + 1, cut), scale, 0)
    tri_ref[...] = jnp.where(
        lax.broadcasted_iota(jnp.int32, (TILE, TILE), 0) > lax.broadcasted_iota(jnp.int32, (TILE, TILE), 1),
        -1.0,
        0.0,
    ).astype(BF16)
    tot_ref[...] = jnp.zeros_like(tot_ref)
    lane = lax.broadcasted_iota(jnp.int32, (len_, LANES), 1)

    def part(to, start, tiles, carry, acc, masked):
        q = qq_ref[to]
        for tile in reversed(range(tiles)):
            keys = pl.ds(pl.multiple_of(start + tile * TILE, TILE), TILE)
            u = dot(q, kk_ref[keys, :], ((1,), (1,))) + off_ref[0:1, keys]
            sp = kept = jnp.maximum(u, jnp.log2(1.0 + jnp.exp2(jnp.minimum(u, 126.0))))
            if masked:
                ahead = lax.broadcasted_iota(jnp.int32, (len_, TILE), 0) - lax.broadcasted_iota(
                    jnp.int32, (len_, TILE), 1
                )
                strict = ahead > start + tile * TILE - x * len_
                kept = jnp.where(strict, sp, 0.0)
            w = dot(kept.astype(BF16), tri_ref[...])
            if carry is None:
                p = jnp.exp2(u - sp + w)
            else:
                p = jnp.exp2(u - sp + w + jnp.concatenate([carry] * (TILE // LANES), axis=1))
            if masked:
                p = jnp.where(strict, p, 0.0)
            summed = dot(p.astype(BF16), v_ref[keys, :])
            total = jnp.broadcast_to(w[:, 0:1] - kept[:, 0:1], (len_, LANES))
            acc = summed if acc is None else acc + summed
            carry = total if carry is None else carry + total
        out_ref[to, pl.ds(0, len_), :] = acc.astype(BF16)
        tot_ref[...] = jnp.where(lane == to, carry, tot_ref[...])
        return carry, acc

    def full(i, done):
        part(i, 0, 2 * half // TILE, None, None, False)
        return done

    def clear(i, done):
        out_ref[i, pl.ds(0, len_), :] = jnp.zeros((len_, hd), BF16)
        return done

    if not rest:
        own = x * len_ // half
        carry_ref[...], acc_ref[...] = part(z, own * half, half // TILE, None, None, True)

        @pl.when(own == 1)
        def _():
            part(z, 0, half // TILE, carry_ref[...], acc_ref[...], False)

        lax.fori_loop(0, z, clear, 0)
    lax.fori_loop(low, high, full, 0)
    cols = [tot_ref[r * LANES : (r + 1) * LANES, :].T for r in range(n_off)]
    for to in range(cut if rest else 0, depth):
        left = [col[to : to + 1, :] for col in cols]
        terms = []
        for _ in range(3):
            term = [r.astype(BF16).astype(F32) for r in left]
            left = [r - t for r, t in zip(left, term)]
            terms += term
        terms.append(jnp.zeros((16 - len(terms), LANES), F32))

        @pl.when(jnp.logical_or(not rest, to > z))
        def _():
            out_ref[to, pl.ds(len_, 16), :] = jnp.concatenate(terms, axis=0).astype(BF16)


def join_kernel(depth, len_, in_ref, out_ref, scale_ref):
    n_off = len_ // LANES
    later = [jnp.zeros((1, LANES), F32)] * n_off
    scale_ref[...] = jnp.zeros_like(scale_ref)
    for at in reversed(range(depth)):
        t = in_ref[at, pl.ds(len_, 16), :].astype(F32)
        for r in range(n_off):
            scale_ref[at : at + 1, r * LANES : (r + 1) * LANES] = jnp.exp2(later[r])
            for term in range(3):
                i = term * n_off + r
                later[r] = later[r] + t[i : i + 1, :]
    for r in range(n_off):
        rows = slice(r * LANES, (r + 1) * LANES)
        cols = scale_ref[:, rows].T
        acc = jnp.zeros((LANES, out_ref.shape[1]), F32)
        for at in range(depth):
            acc = acc + in_ref[at, rows, :].astype(F32) * cols[:, at : at + 1]
        out_ref[rows, :] = acc.astype(out_ref.dtype)


def vmem(n):
    return [pl.BlockSpec(memory_space=pltpu.VMEM)] * n


SMEM = pl.BlockSpec(memory_space=pltpu.SMEM)


def dispatch_kernel(cap, at_ref, rows_ref, gain_ref, ids_ref, wts_ref, out_ref, hi_ref, lo_ref):
    tok, slots = rows_ref.shape[0], out_ref.shape[0]
    rows = rows_ref[...].astype(F32)
    rms = lax.rsqrt(jnp.mean(rows * rows, axis=1, keepdims=True) + EPSILON)
    first, second = ids_ref[0:1, :], ids_ref[1:2, :]
    expert = lax.broadcasted_iota(jnp.int32, (LANES, tok), 0)
    chosen = jnp.where((first == expert) | (second == expert), 1.0, 0.0).astype(BF16)
    before = lax.broadcasted_iota(jnp.int32, (tok, tok), 0) < lax.broadcasted_iota(
        jnp.int32, (tok, tok), 1
    )
    rank = dot(chosen, jnp.where(before, 1.0, 0.0).astype(BF16)).astype(BF16)
    spread = (
        lax.broadcasted_iota(jnp.int32, (slots, LANES), 0) // cap
        == lax.broadcasted_iota(jnp.int32, (slots, LANES), 1)
    )
    spread = jnp.where(spread, 1.0, 0.0).astype(BF16)
    slot = lax.broadcasted_iota(jnp.int32, (slots, tok), 0)
    taken = (dot(spread, chosen) > 0.5) & (dot(spread, rank) == (slot % cap).astype(F32))
    pick = jnp.where(taken, 1.0, 0.0).astype(BF16)
    for i in range(out_ref.shape[1] // LANES):
        own = pl.ds(pl.multiple_of((2 * i + at_ref[0]) * LANES, LANES), LANES)
        normed = (rows_ref[:, own].astype(F32) * rms * gain_ref[:, own]).astype(BF16)
        out_ref[:, i * LANES : (i + 1) * LANES] = dot(pick, normed).astype(BF16)
    weight = jnp.where(slot // cap == first, wts_ref[0:1, :], wts_ref[1:2, :])
    weight = jnp.where(taken, weight, 0.0)
    hi = weight.astype(BF16)
    hi_ref[...] = hi
    lo_ref[...] = (weight - hi.astype(F32)).astype(BF16)


def expert_kernel(at_ref, mine_ref, other_ref, gate_ref, up_ref, down_ref, keep_ref, send_ref, all_ref):
    core = at_ref[0]
    chunks = mine_ref.shape[1] // LANES
    for i in range(chunks):
        here = slice(i * LANES, (i + 1) * LANES)
        all_ref[:, pl.ds(pl.multiple_of((2 * i + core) * LANES, LANES), LANES)] = mine_ref[:, here]
        all_ref[:, pl.ds(pl.multiple_of((2 * i + 1 - core) * LANES, LANES), LANES)] = other_ref[:, here]
    tokens = all_ref[...]
    gate = dot(tokens, gate_ref[...], ((1,), (1,)))
    up = dot(tokens, up_ref[...], ((1,), (1,)))
    hidden = (gate / (1.0 + jnp.exp(-gate)) * up).astype(BF16)
    all_ref[...] = dot(hidden, down_ref[...]).astype(BF16)
    for i in range(chunks):
        keep_ref[i] = all_ref[:, pl.ds(pl.multiple_of((2 * i + core) * LANES, LANES), LANES)]
        send_ref[i] = all_ref[:, pl.ds(pl.multiple_of((2 * i + 1 - core) * LANES, LANES), LANES)]


def combine_kernel(hi_ref, lo_ref, back_ref, out_ref):
    back = back_ref[...]
    out_ref[...] = (
        dot(hi_ref[...], back, ((0,), (0,))) + dot(lo_ref[...], back, ((0,), (0,)))
    ).astype(BF16)


def swap(x):
    return lax.ppermute(x, "core", [(0, 1), (1, 0)])


def layer(
    queries, keys, values, key_offset, rows, gain, gate_w, up_w, down_w, expert_ids, route_weights
):
    experts = lax.axis_size(EP)
    tok, width = rows.shape
    half = width // lax.axis_size("core")
    hosts = lax.axis_size("y")
    cap = 2 * expert_ids.shape[1] * tok // experts
    slots = experts * cap
    depth, wide = lax.axis_size(Z), lax.axis_size("x")
    len_, hd = queries.shape
    core = jnp.stack([lax.axis_index("core")]).astype(jnp.int32)
    place = jnp.stack([lax.axis_index(Z), lax.axis_index("x")]).astype(jnp.int32)
    outgoing, hi, lo = pl.pallas_call(
        functools.partial(dispatch_kernel, cap),
        out_shape=(
            jax.ShapeDtypeStruct((slots, half), BF16),
            jax.ShapeDtypeStruct((slots, tok), BF16),
            jax.ShapeDtypeStruct((slots, tok), BF16),
        ),
        in_specs=[SMEM] + vmem(4),
        out_specs=tuple(vmem(3)),
        name="dispatch",
    )(core, rows, gain.reshape(1, -1), expert_ids.T, route_weights.T)
    mine = lax.all_to_all(outgoing.reshape(experts, cap, half), EP, 0, 0, tiled=True)
    mine = mine.reshape(slots, half)

    off = jnp.pad(key_offset.reshape(-1, LANES), ((0, 16 - len_ // LANES), (0, 0)))
    kvo = [jnp.concatenate([keys, values, off], axis=0)]
    for step in range(1, wide):
        kvo.append(lax.ppermute(kvo[0], "x", [(i, (i + step) % wide) for i in range(wide)]))
    q = lax.ppermute(queries, "zl", [(0, 1), (1, 0)])
    q = jnp.concatenate([queries, q], axis=0)
    q = lax.all_gather(q, "zh").reshape(depth, len_, hd)

    hidden = gate_w.shape[2]
    other = swap(mine)
    keep, send = pl.pallas_call(
        expert_kernel,
        out_shape=(jax.ShapeDtypeStruct((hosts, slots, LANES), BF16),) * 2,
        in_specs=[SMEM] + vmem(5),
        out_specs=tuple(vmem(2)),
        scratch_shapes=[pltpu.VMEM((slots, width), BF16)],
        compiler_params=pltpu.CompilerParams(vmem_limit_bytes=32 << 20),
        cost_estimate=pl.CostEstimate(
            flops=6 * slots * width * hidden,
            transcendentals=slots * hidden,
            bytes_accessed=2 * (2 * slots * width + 3 * width * hidden),
        ),
        name="experts",
    )(core, mine, other, gate_w[0].T, up_w[0].T, down_w[0])
    other = swap(send)
    share = (keep.astype(F32) + other.astype(F32)).astype(BF16)
    share = lax.all_to_all(share, "y", 0, 0, tiled=True)

    def blocks(rest, *prev):
        share_of = (depth - cut if rest else cut) / depth
        return pl.pallas_call(
            functools.partial(block_kernel, depth, wide, len_, hd, cut, rest),
            out_shape=jax.ShapeDtypeStruct((depth, len_ + 16, hd), BF16),
            in_specs=[SMEM] + vmem(1 + len(prev) + wide),
            out_specs=vmem(1)[0],
            scratch_shapes=[
                pltpu.VMEM((depth, len_, 2 * hd), BF16),
                pltpu.VMEM((wide * len_, 2 * hd), BF16),
                pltpu.VMEM((wide * len_, hd), BF16),
                pltpu.VMEM((8, wide * len_), F32),
                pltpu.VMEM((TILE, TILE), BF16),
                pltpu.VMEM((len_, LANES), F32),
                pltpu.VMEM((len_, hd), F32),
                pltpu.VMEM((len_, LANES), F32),
            ],
            compiler_params=pltpu.CompilerParams(vmem_limit_bytes=32 << 20),
            cost_estimate=pl.CostEstimate(
                flops=int(share_of * depth * wide * len_ * len_ * (4 * hd + 2 * len_)),
                transcendentals=int(share_of * 3 * depth * wide * len_ * len_),
                bytes_accessed=2 * (2 * depth * len_ * hd + wide * kvo[0].size),
            ),
            name="stick_rest" if rest else "stick_first",
        )(place, q, *prev, *kvo)

    cut = depth * 5 // 8
    sums = blocks(True, blocks(False))
    arrived = lax.all_to_all(sums, Z, 0, 0, tiled=True)
    attended = pl.pallas_call(
        functools.partial(join_kernel, depth, len_),
        out_shape=jax.ShapeDtypeStruct((len_, hd), BF16),
        in_specs=vmem(1),
        out_specs=vmem(1)[0],
        scratch_shapes=[pltpu.VMEM((LANES, len_), F32)],
        cost_estimate=pl.CostEstimate(
            flops=2 * depth * len_ * hd, transcendentals=depth * len_, bytes_accessed=2 * depth * len_ * hd
        ),
        name="stick_join",
    )(arrived)

    share = share.astype(F32).sum(axis=0).astype(BF16)
    back = lax.all_to_all(share.reshape(experts, cap, LANES), EP, 0, 0, tiled=True)
    mixed = pl.pallas_call(
        combine_kernel,
        out_shape=jax.ShapeDtypeStruct((tok, LANES), BF16),
        in_specs=vmem(3),
        out_specs=vmem(1)[0],
        name="combine",
    )(hi, lo, back.reshape(slots, LANES))
    mixed = lax.all_gather(mixed, TP, axis=1, tiled=True)
    return (attended, mixed)


def solution(mesh):
    fine = Mesh(mesh.devices.reshape(ZH, ZL, X, Y, CORE), (*Z, "x", *TP))
    return jax.shard_map(
        layer,
        mesh=fine,
        in_specs=(
            P(EP, TP),
            P(EP, TP),
            P(EP, TP),
            P(EP, TP),
            P(EP, None),
            P(),
            P(EP, None, TP),
            P(EP, None, TP),
            P(EP, TP, None),
            P(EP, None),
            P(EP, None),
        ),
        out_specs=(P(EP, TP), P(EP, None)),
        check_vma=False,
    )
```
